32 devices in a mesh: ep: 8 (over z, x), tp: 4 (over y, core).
Axes of the slice: x: 2, y: 2, z: 4, core: 2. Of those that a mesh axis runs over, the one named last changes fastest.
Arguments:
- mixer_rows: bfloat16 [2048, 4096], P('ep'), may hold values from -8 to 8, as said below
- mixer_gain: float32 [4096], replicated, may hold values from 0.1 to 1.9
- gate_proj: bfloat16 [4096, 4096], P(None, 'tp'), may hold values from -0.09375 to 0.09375
- input_proj: bfloat16 [4096, 4096], P(None, 'tp'), may hold values from -0.09375 to 0.09375
- conv_taps: float32 [4, 4096], P(None, 'tp'), may hold values from -2 to 2
- input_gates: bfloat16 [16, 256, 256], P('tp'), may hold values from -0.375 to 0.375
- decay_gates: bfloat16 [16, 256, 256], P('tp'), may hold values from -0.375 to 0.375
- decay_offset: float32 [4096], P('tp'), may hold values from 4.8 to 13, as said below
- out_proj: bfloat16 [4096, 4096], P('tp'), may hold values from -0.09375 to 0.09375
- mixer_scale: float32 [4096], replicated, may hold values from 0.1 to 1.9
- expert_rows: bfloat16 [2048, 4096], P('ep'), may hold values from -6 to 6
- expert_gain: float32 [4096], replicated, may hold values from 0.1 to 1.9
- route_ids: int32 [2048, 2], P('ep'), may hold values from 0 to 7, all different within a row; in each aligned block of 256 rows (0 to 255, 256 to 511, ...) at most 96 rows name the same one
- route_weights: float32 [2048, 2], P('ep'), may hold values from 0.5 to 2
- expert_gate: bfloat16 [8, 4096, 1024], P('ep', None, 'tp'), may hold values from -0.09375 to 0.09375
- expert_up: bfloat16 [8, 4096, 1024], P('ep', None, 'tp'), may hold values from -0.09375 to 0.09375
- expert_down: bfloat16 [8, 1024, 4096], P('ep', 'tp'), may hold values from -0.1875 to 0.1875
- shared_gate: bfloat16 [4096, 1024], P(None, 'tp'), may hold values from -0.09375 to 0.09375
- shared_up: bfloat16 [4096, 1024], P(None, 'tp'), may hold values from -0.09375 to 0.09375
- shared_down: bfloat16 [1024, 4096], P('tp'), may hold values from -0.1875 to 0.1875
- expert_scale: float32 [4096], replicated, may hold values from 0.1 to 1.9
Outputs:
- mixer_out: bfloat16 [2048, 4096], P(('ep', 'tp'))
- expert_out: bfloat16 [2048, 4096], P(('ep', 'tp'))
The draws below stay inside these ranges and needn't reach their ends.
Inputs may be any that keep to these rules, and one draw needn't show every extreme that they name: `mixer_rows`: order one, with a common direction whose weight drifts slowly along the sequence. `decay_offset`: the even channels forget within some 30 to 200 tokens; the odd channels keep 5 to 90 percent of their state over the whole sequence of 2048 tokens. `route_ids`: each row names 2 different experts; within the rows of one index of ep (aligned blocks of 256 rows) no expert is named by more than 96 rows, and in some blocks one is named by exactly 96.
All inputs are finite; a program needn't handle non-finite values.
Results may differ from the reference program's by a relative error of at most 0.0033.
The reference program's roundings to bfloat16 on the way count: a program that leaves them out, or rounds other values in their place, can miss the bound.
Values may be sent and summed in bfloat16 or wider, within the bound.
A program may use at most 192 MiB of HBM per device.

```python
import math
import jax
import jax.numpy as jnp
import numpy as np
from jax import lax

D = 4096
RNN_BLOCKS = 16
BLOCK_WIDTH = 256
CONV = 4
EXPERT_HIDDEN = 1024
SHARED_HIDDEN = 1024
TOP_K = 2
ROWS = 256
EXPERTS = 8
TOKENS = 2048
CAP = 96
N_EP = 8


def draw_mixer_rows(key, part):
    noise_key, direction_key, phase_key = jax.random.split(key, 3)
    noise_part = jax.random.normal(noise_key, (TOKENS, D), jnp.float32)
    direction = jax.random.normal(direction_key, (D,), jnp.float32)
    phase_shift = jax.random.uniform(phase_key, (), jnp.float32, 0.0, 2.0 * math.pi)
    positions = jnp.arange(TOKENS, dtype=jnp.float32) / TOKENS
    drift_level = 2.0 * jnp.sin(3.0 * math.pi * positions + phase_shift)
    values = noise_part + drift_level[:, None] * direction[None, :]
    return jnp.clip(values, -8.0, 8.0).astype(jnp.bfloat16)


def draw_decay_offset(key, part):
    fast_key, slow_key = jax.random.split(key)
    fast_part = jax.random.uniform(fast_key, (D,), jnp.float32, 4.8, 6.7)
    slow_part = math.log(TOKENS) + jax.random.uniform(slow_key, (D,), jnp.float32, 0.3, 3.6)
    parity = jnp.arange(D) % 2
    return jnp.where(parity == 0, fast_part, slow_part).astype(jnp.float32)


def levels(key, dims, pieces, least, high):
    gain = 1.0
    for axis_at, shards_of in pieces:
        heights = jax.random.uniform(jax.random.fold_in(jax.random.fold_in(key, 6), axis_at), (shards_of,), jnp.float32, least / len(pieces), high / len(pieces))
        gain = gain * jnp.repeat(jnp.exp(heights), dims[axis_at] // shards_of).reshape((-1,) + (1,) * (len(dims) - 1 - axis_at))
    return gain


def routed_block(key, own, number, rows, amount, top, most, skew):
    order = jax.random.permutation(key, amount)
    crowded, common = portions_of(amount, rows * top, most, skew, True), portions_of(amount, rows * top, most, skew, False)
    places = jnp.arange(amount)

    def named(lengths, offset_by):
        used = int((lengths > 0).sum())
        fixed = max(1, used // 4)
        shifted = fixed + (places - fixed + offset_by * (used - fixed)) % max(1, amount - fixed)
        return jnp.zeros((amount,), jnp.int32).at[order[jnp.where(places < fixed, places, shifted)]].set(jnp.asarray(lengths, jnp.int32))

    lengths = jnp.where(number % 4 == 0, named(crowded, number // 4), named(common, number - number // 4 - 1))
    mixed = jax.random.permutation(jax.random.fold_in(own, 3), amount)
    donor, sink = mixed[0:amount // 2 * 2:2], mixed[1:amount // 2 * 2:2]
    room = jnp.minimum(lengths[donor] - 1, most - lengths[sink]) // 2
    room = jnp.where((donor == order[0]) | (sink == order[0]) | (lengths[sink] == 0), 0, jnp.maximum(room, 0))
    shifted = jax.random.randint(jax.random.fold_in(own, 4), (amount // 2,), 0, 1 << 20) % (room + 1)
    lengths = lengths.at[donor].add(-shifted).at[sink].add(shifted)
    members = jnp.searchsorted(jnp.cumsum(lengths), jnp.arange(rows * top), side="right").astype(jnp.int32)
    listing = members.reshape(top, rows).T
    listing = listing[jax.random.permutation(jax.random.fold_in(own, 1), rows)]
    offset_by = jax.random.randint(jax.random.fold_in(own, 2), (rows, 1), 0, top)
    return jnp.take_along_axis(listing, (jnp.arange(top)[None, :] + offset_by) % top, axis=1)


def portions_of(amount, total, bound, slope, full):
    portions = [(1 << 20) // math.isqrt(standing ** slope) + 1 for standing in range(1, amount + 1)]
    largest = bound if full else min(bound, max(-(-total // amount), total * portions[0] // sum(portions)))
    least = 1 if total - largest >= amount - 1 else 0
    counts, spare = [largest] + [least] * (amount - 1), total - largest - least * (amount - 1)
    while spare > 0:
        free = [i for i in range(1, amount) if counts[i] < largest] or [i for i in range(1, amount) if counts[i] < bound]
        whole, budget = sum([portions[i] for i in free]), spare
        for i in free:
            more = min(bound - counts[i], max(1, budget * portions[i] // whole), spare)
            counts[i] = counts[i] + more
            spare = spare - more
    return np.array(counts)


def centred(stream_key, shape, deviation, reach, cuts=(), kind=jnp.bfloat16):
    array = jax.random.normal(stream_key, shape, jnp.float32) * deviation
    if len(cuts) > 0:
        array = levels(stream_key, shape, cuts, -0.22, 0.18) * array
    return jnp.clip(array, min=-reach, max=reach).astype(kind)


def setup_inputs(seed: int = 0) -> dict:
    keys = jax.random.split(jax.random.key(seed), 22)
    mixer_rows = draw_mixer_rows(jax.random.fold_in(keys[21], 71), 0)
    mixer_gain = jnp.clip(1.0 + 0.18 * jax.random.normal(keys[1], (D,), jnp.float32), 0.1, 1.9)
    gate_proj = centred(keys[2], (D, D), D ** -0.5, 0.09375, ((1, 4),))
    input_proj = centred(keys[3], (D, D), D ** -0.5, 0.09375, ((1, 4),))
    conv_taps = centred(keys[4], (CONV, D), 0.5, 2.0, ((1, 4),), jnp.float32)
    input_gates = centred(keys[5], (RNN_BLOCKS, BLOCK_WIDTH, BLOCK_WIDTH), BLOCK_WIDTH ** -0.5, 0.375, ((0, 4),))
    decay_gates = centred(keys[6], (RNN_BLOCKS, BLOCK_WIDTH, BLOCK_WIDTH), BLOCK_WIDTH ** -0.5, 0.375, ((0, 4),))
    decay_offset = draw_decay_offset(jax.random.fold_in(keys[21], 71), 0)
    out_proj = centred(keys[8], (D, D), D ** -0.5, 0.09375, ((0, 4),))
    mixer_scale = jnp.clip(1.0 + 0.18 * jax.random.normal(keys[9], (D,), jnp.float32), 0.1, 1.9)
    expert_rows = centred(keys[10], (TOKENS, D), 1.0, 6.0, ((0, 8),))
    expert_gain = jnp.clip(1.0 + 0.18 * jax.random.normal(keys[11], (D,), jnp.float32), 0.1, 1.9)
    route_ids_keys = jax.random.split(jax.random.fold_in(keys[12], 1), TOKENS // ROWS)
    route_ids_turns = jax.random.permutation(jax.random.fold_in(keys[12], 3), TOKENS // ROWS)
    route_ids = jax.vmap(lambda own, number: routed_block(jax.random.fold_in(keys[12], 2), own, number, ROWS, EXPERTS, TOP_K, CAP, 1))(route_ids_keys, route_ids_turns).reshape((TOKENS, TOP_K))
    route_weights = jnp.clip(0.5 + 1.5 * jax.random.uniform(keys[13], (TOKENS, TOP_K), jnp.float32) ** levels(keys[13], (TOKENS, TOP_K), ((0, 8),), -0.2, 0.2), 0.5, 2.0)
    expert_gate = centred(keys[14], (EXPERTS, D, EXPERT_HIDDEN), D ** -0.5, 0.09375, ((0, 8), (2, 4)))
    expert_up = centred(keys[15], (EXPERTS, D, EXPERT_HIDDEN), D ** -0.5, 0.09375, ((0, 8), (2, 4)))
    expert_down = centred(keys[16], (EXPERTS, EXPERT_HIDDEN, D), EXPERT_HIDDEN ** -0.5, 0.1875, ((0, 8), (1, 4)))
    shared_gate = centred(keys[17], (D, SHARED_HIDDEN), D ** -0.5, 0.09375, ((1, 4),))
    shared_up = centred(keys[18], (D, SHARED_HIDDEN), D ** -0.5, 0.09375, ((1, 4),))
    shared_down = centred(keys[19], (SHARED_HIDDEN, D), SHARED_HIDDEN ** -0.5, 0.1875, ((0, 4),))
    expert_scale = jnp.clip(1.0 + 0.18 * jax.random.normal(keys[20], (D,), jnp.float32), 0.1, 1.9)
    return dict(mixer_rows=mixer_rows, mixer_gain=mixer_gain, gate_proj=gate_proj, input_proj=input_proj, conv_taps=conv_taps, input_gates=input_gates, decay_gates=decay_gates, decay_offset=decay_offset, out_proj=out_proj, mixer_scale=mixer_scale, expert_rows=expert_rows, expert_gain=expert_gain, route_ids=route_ids, route_weights=route_weights, expert_gate=expert_gate, expert_up=expert_up, expert_down=expert_down, shared_gate=shared_gate, shared_up=shared_up, shared_down=shared_down, expert_scale=expert_scale)


eps = 1e-06
lru_power = 8.0

def rms_scale(values, scale):
    floats = values.astype(jnp.float32)
    return floats * lax.rsqrt(lax.optimization_barrier(jnp.mean(floats * floats, axis=-1, keepdims=True)) + eps) * scale

def linear_pair(earlier, later):
    return (earlier[0] * later[0], later[0] * earlier[1] + later[1])

def slot_table(route_ids, expert_count, capacity):
    id_list = route_ids.reshape(-1).astype(jnp.int32)
    indicator = (id_list[:, None] == jnp.arange(expert_count, dtype=jnp.int32)[None, :]).astype(jnp.int32)
    earlier_count = (jnp.cumsum(indicator, axis=0).astype(jnp.int32) - indicator).astype(jnp.int32)
    position = lax.optimization_barrier(jnp.sum(earlier_count * indicator, axis=1)).astype(jnp.int32)
    slot_ids = (id_list * capacity + position).astype(jnp.int32)
    matched = (slot_ids[None, :] == jnp.arange(expert_count * capacity, dtype=jnp.int32)[:, None]).astype(jnp.int32)
    source = lax.optimization_barrier(jnp.sum(matched * jnp.arange(id_list.shape[0], dtype=jnp.int32)[None, :], axis=1)).astype(jnp.int32)
    filled = lax.optimization_barrier(jnp.sum(matched, axis=1)) > 0
    return (slot_ids, source, filled)

def mixer_half(mixer_rows, mixer_gain, gate_proj, input_proj, conv_taps, input_gates, decay_gates, decay_offset, out_proj, mixer_scale):
    row_count = mixer_rows.shape[0]
    normed = rms_scale(mixer_rows, mixer_gain).astype(jnp.bfloat16)
    gate_branch = jax.nn.gelu(jnp.dot(normed, gate_proj, preferred_element_type=jnp.float32))
    branch = jnp.dot(normed, input_proj, preferred_element_type=jnp.float32).astype(jnp.bfloat16)
    tap_count = conv_taps.shape[0]
    padded = jnp.concatenate([jnp.zeros((tap_count - 1, branch.shape[1]), branch.dtype), branch], axis=0)
    conv_sum = conv_taps[0] * padded[0:row_count].astype(jnp.float32)
    for tap_index in range(1, tap_count):
        conv_sum = conv_sum + conv_taps[tap_index] * padded[tap_index:tap_index + row_count].astype(jnp.float32)
    conv_out = conv_sum.astype(jnp.bfloat16)
    block_rows = conv_out.astype(jnp.float32).reshape(row_count, input_gates.shape[0], input_gates.shape[1])
    input_gate = jax.nn.sigmoid(jnp.einsum('rbi,bij->rbj', block_rows, input_gates.astype(jnp.float32))).reshape(row_count, -1)
    decay_gate = jax.nn.sigmoid(jnp.einsum('rbi,bij->rbj', block_rows, decay_gates.astype(jnp.float32))).reshape(row_count, -1)
    log_decay = -lru_power * decay_gate * jax.nn.softplus(-decay_offset)
    positions = jnp.arange(row_count, dtype=jnp.int32)
    input_scale = jnp.where((positions == 0)[:, None], 1.0, jnp.sqrt(-jnp.expm1(2.0 * log_decay)))
    drive_term = input_scale * input_gate * conv_out.astype(jnp.float32)
    decay_product, states = lax.associative_scan(linear_pair, (jnp.exp(log_decay), drive_term), axis=0)
    gated_rows = (gate_branch * states).astype(jnp.bfloat16)
    mixer_sum = jnp.dot(gated_rows, out_proj, preferred_element_type=jnp.float32)
    return rms_scale(mixer_sum, mixer_scale).astype(jnp.bfloat16)

def expert_half(expert_rows, expert_gain, route_ids, route_weights, expert_gate, expert_up, expert_down, shared_gate, shared_up, shared_down, expert_scale):
    expert_normed = rms_scale(expert_rows, expert_gain).astype(jnp.bfloat16)
    expert_count = expert_gate.shape[0]
    top_count = route_ids.shape[1]
    row_width = expert_rows.shape[1]
    gate_whole = expert_gate.astype(jnp.float32)
    up_whole = expert_up.astype(jnp.float32)
    down_whole = expert_down.astype(jnp.float32)

    def one_block(inputs):
        block_rows, block_ids, block_weights = inputs
        slot_ids, source, filled = slot_table(block_ids, expert_count, CAP)
        outgoing = jnp.where(filled[:, None], block_rows[source // top_count], jnp.zeros((), block_rows.dtype))
        outgoing = outgoing.reshape(expert_count, CAP, row_width).astype(jnp.float32)
        gate_part = jnp.einsum('ecd,edf->ecf', outgoing, gate_whole)
        up_part = jnp.einsum('ecd,edf->ecf', outgoing, up_whole)
        copy_hidden = (jax.nn.silu(gate_part) * up_part).astype(jnp.bfloat16)
        results = jnp.einsum('ecf,efd->ecd', copy_hidden.astype(jnp.float32), down_whole)
        picked = results.reshape(expert_count * CAP, row_width)[slot_ids] * block_weights.reshape(-1, 1)
        return lax.optimization_barrier(jnp.sum(picked.reshape(ROWS, top_count, row_width), axis=1))
    routed = lax.map(one_block, (expert_normed.reshape(N_EP, ROWS, row_width), route_ids.reshape(N_EP, ROWS, top_count), route_weights.reshape(N_EP, ROWS, top_count)))
    routed = routed.reshape(expert_rows.shape[0], row_width)
    shared_hidden = (jax.nn.silu(jnp.dot(expert_normed, shared_gate, preferred_element_type=jnp.float32)) * jnp.dot(expert_normed, shared_up, preferred_element_type=jnp.float32)).astype(jnp.bfloat16)
    expert_sum = routed + jnp.dot(shared_hidden, shared_down, preferred_element_type=jnp.float32)
    return rms_scale(expert_sum, expert_scale).astype(jnp.bfloat16)

def reference(mixer_rows, mixer_gain, gate_proj, input_proj, conv_taps, input_gates, decay_gates, decay_offset, out_proj, mixer_scale, expert_rows, expert_gain, route_ids, route_weights, expert_gate, expert_up, expert_down, shared_gate, shared_up, shared_down, expert_scale):
    mixer_out = mixer_half(mixer_rows, mixer_gain, gate_proj, input_proj, conv_taps, input_gates, decay_gates, decay_offset, out_proj, mixer_scale)
    expert_out = expert_half(expert_rows, expert_gain, route_ids, route_weights, expert_gate, expert_up, expert_down, shared_gate, shared_up, shared_down, expert_scale)
    return (mixer_out, expert_out)
```

```python
import functools

import jax
import jax.numpy as jnp
from jax import lax
from jax.experimental import pallas as pl
from jax.experimental.pallas import tpu as pltpu
from jax.sharding import PartitionSpec as P

eps = 1e-06
lru_power = 8.0
halo_rows = 16
MESH = pl.DeviceIdType.MESH
f32 = jnp.float32
bf16 = jnp.bfloat16


def rms_scale(values, scale):
    floats = values.astype(f32)
    return floats * lax.rsqrt(jnp.mean(floats * floats, axis=-1, keepdims=True) + eps) * scale


def remote(src, dst, send_sem, recv_sem, ep_at, tp_at):
    return pltpu.make_async_remote_copy(
        src_ref=src,
        dst_ref=dst,
        send_sem=send_sem,
        recv_sem=recv_sem,
        device_id=(ep_at, tp_at),
        device_id_type=MESH,
    )


def greet(peers):
    barrier = pltpu.get_barrier_semaphore()
    for ep_at, tp_at in peers:
        pl.semaphore_signal(barrier, inc=1, device_id=(ep_at, tp_at), device_id_type=MESH)
    pl.semaphore_wait(barrier, len(peers))


def expm1_neg(y):
    series = y * (1 + y / 2 * (1 + y / 3 * (1 + y / 4 * (1 + y / 5 * (1 + y / 6 * (1 + y / 7))))))
    return jnp.where(y > -0.35, series, jnp.exp(y) - 1.0)


def softplus_neg(x):
    u = jnp.exp(-jnp.abs(x))
    series = u * (1 - u * (1 / 2 - u * (1 / 3 - u * (1 / 4 - u * (1 / 5 - u / 6)))))
    return jnp.maximum(-x, 0.0) + jnp.where(u < 0.05, series, jnp.log(1.0 + u))


def layer_kernel(
    ep, tp, top,
    ids_ref, weights_ref, taps_ref, ig_ref, dg_ref, offset_ref, mg_ref, xg_ref, ms_ref, es_ref,
    rows_hbm, tokens_hbm, ip_hbm, gp_hbm, op_hbm, eg_hbm, eu_hbm, ed, sg_hbm, su_hbm, sd_hbm,
    mo_ref, eo_ref,
    outq, normed, en, e_out, r_out, r_near,
    w1, eg, eu, wd, sd, recv, hid, ret, back, mt, st, m_half, e_half, m_out, m_in, e_in,
    r_buf, r_in, total, gate, a_buf, b_buf, ext, ends, got, gated, meta, cols_ref,
    load_sem, halo_send, halo_recv, end_send, end_recv,
    z_s, z_r, y_s, y_r, c_s, c_r, hy_s, hy_r, hc_s, hc_r, w_s, w_r, b_s, b_r,
    md_s, md_r, ed_s, ed_r, my_s, my_r, ey_s, ey_r, r_s, r_r,
):
    me, t = lax.axis_index("ep"), lax.axis_index("tp")
    ys = tp // 2
    y, c = t // 2, lax.rem(t, 2)
    mate = y * 2 + 1 - c
    dq = outq.shape[3]
    cap = outq.shape[2]
    rows, width = ext.shape[0] - halo_rows, ext.shape[1]
    each = rows // tp
    blocks, bw = ig_ref.shape[0], ig_ref.shape[1]
    sh_width = sd.shape[0]
    half, quarter = ep // 2, ep // 4
    groups = ep // 2
    inner = lax.rem(me // quarter + 1, 4) // 2

    def at_y(k):
        return lax.rem(y + k, ys)

    def up(k):
        return at_y(k) * 2 + c

    def down_of(k, core):
        return lax.rem(y + ys - k, ys) * 2 + core

    def partner(i):
        out, bit = 0, 1
        while bit < ep:
            out = out + lax.rem(me // bit + i // bit, 2) * bit
            bit *= 2
        return out

    def far(j):
        return half + lax.rem(j + inner * quarter, half)

    def base_of(g):
        return 2 * g if 2 * g < half else far(2 * g - half)

    def blocks_of(g):
        base = base_of(g)
        return [i for i in (base, base + 1) if not (isinstance(i, int) and i == 0)]

    def load(src, dst, at):
        return pltpu.make_async_copy(src, dst, load_sem.at[at])

    tokens_load, rows_load = load(tokens_hbm, en, 0), load(
        rows_hbm, normed.at[pl.ds(halo_rows, rows)], 9 + tp
    )
    tokens_load.start()
    rows_load.start()
    ip_load = load(ip_hbm, w1, 1)
    ip_load.start()

    greet(
        [(lax.rem(me + i, ep), t) for i in range(1, ep)]
        + [(me, lax.rem(t + i, tp)) for i in range(1, tp)]
    )

    def z_copy(i, yy):
        return remote(
            outq.at[yy, i], recv.at[yy * 2 + c, i], z_s.at[yy, i], z_r.at[yy, i], partner(i), t
        )

    def y_copy(k, i):
        return remote(recv.at[t, i], recv.at[t, i], y_s.at[k, i], y_r.at[k, i], me, up(k))

    def c_copy(k, i):
        q = down_of(k, c)
        return remote(recv.at[q, i], recv.at[q, i], c_s.at[k, i], c_r.at[k, i], me, mate)

    def hy_copy(k, g):
        part = hid.at[t, pl.ds(base_of(g), 2)]
        return remote(part, part, hy_s.at[k, g], hy_r.at[k, g], me, up(k))

    def hc_copy(k, g):
        part = hid.at[down_of(k, c), pl.ds(base_of(g), 2)]
        return remote(part, part, hc_s.at[k, g], hc_r.at[k, g], me, mate)

    def w_copy(i):
        q = lax.rem(t + i, tp)
        return remote(
            ed.at[:, pl.ds(pl.multiple_of(q * dq, dq), dq)], wd.at[t],
            w_s.at[i], w_r.at[i], me, q,
        )

    def b_copy(i):
        return remote(ret.at[i], back.at[i], b_s.at[i], b_r.at[i], partner(i), t)

    def halo_copy():
        return remote(
            rows_hbm.at[pl.ds(rows - halo_rows, halo_rows)], normed.at[pl.ds(0, halo_rows)],
            halo_send, halo_recv, lax.rem(me + 1, ep), t,
        )

    def end_copy(i):
        return remote(ends, got.at[i], end_send.at[i], end_recv.at[i], lax.rem(me + i, ep), t)

    def pair(ref, half, s, r, k):
        return remote(ref.at[at_y(k) * 2 + 1 - c], half.at[k], s.at[k], r.at[k], me, mate)

    def my_copy(k):
        return remote(m_out.at[k], m_in.at[k], my_s.at[k], my_r.at[k], me, up(k))

    def ey_copy(k):
        return remote(e_out.at[k], e_in.at[k], ey_s.at[k], ey_r.at[k], me, up(k))

    def r_copy(k, core):
        j, q = 2 * k + core, at_y(k) * 2 + lax.rem(c + core, 2)
        if k == 0:
            return remote(r_buf.at[q], r_near, r_s.at[j], r_r.at[j], me, q)
        return remote(r_out.at[q], r_in.at[t], r_s.at[j], r_r.at[j], me, q)

    def normalize(ref, gain):
        def some(r, _):
            at = pl.ds(pl.multiple_of(r * 16, 16), 16)
            ref[at, :] = rms_scale(ref[at, :], gain[...]).astype(bf16)
            return 0

        lax.fori_loop(0, ref.shape[0] // 16, some, 0)

    halo_copy().start()
    member = lax.broadcasted_iota(jnp.int32, (ep, rows), 0)
    chosen = [
        (jnp.bitwise_xor(ids_ref[k : k + 1, :], me) == member).astype(f32) for k in range(top)
    ]
    named = chosen[0]
    for k in range(1, top):
        named = named + chosen[k]
    before = lax.broadcasted_iota(jnp.int32, (rows, rows), 0) < lax.broadcasted_iota(
        jnp.int32, (rows, rows), 1
    )
    earlier = jnp.dot(
        named.astype(bf16), before.astype(f32).astype(bf16), preferred_element_type=f32
    )
    spots = earlier + member.astype(f32) * cap
    meta[...] = jnp.zeros_like(meta)
    for k in range(top):
        meta[k : k + 1, :] = jnp.sum(chosen[k] * spots, axis=0, keepdims=True)
        meta[top + k : top + k + 1, :] = weights_ref[k : k + 1, :]
    cols_ref[...] = meta[...].T

    tokens_load.wait()
    for i in range(1, tp):
        w_copy(i).start()
    eg_load, eu_load = load(eg_hbm, eg, 2), load(eu_hbm, eu, 3)
    eg_load.start()
    eu_load.start()
    wd_load = load(ed.at[:, pl.ds(pl.multiple_of(t * dq, dq), dq)], wd.at[t], 4)
    wd_load.start()
    sd_load = load(sd_hbm, sd, 5)
    sd_load.start()
    normalize(en, xg_ref)
    mine = pl.ds(pl.multiple_of(t * dq, dq), dq)

    def place(i):
        spot = (lax.broadcasted_iota(jnp.int32, (cap, rows), 0) + i * cap).astype(f32)
        hot = meta[0:1, :] == spot
        for k in range(1, top):
            hot = hot | (meta[k : k + 1, :] == spot)
        return hot.astype(f32).astype(bf16)

    def dispatch_near(i, _):
        hot = place(i)
        for yy in range(ys):
            part = pl.ds(pl.multiple_of((yy * 2 + c) * dq, dq), dq)
            outq[yy, i] = jnp.dot(hot, en[:, part], preferred_element_type=f32).astype(bf16)
            z_copy(i, yy).start()
        return 0

    def dispatch_far(j, _):
        i = far(j)
        outq[y, i] = jnp.dot(place(i), en[:, mine], preferred_element_type=f32).astype(bf16)
        z_copy(i, y).start()
        return 0

    def dispatch_fars(when, lo, hi):
        @pl.when(inner == when)
        def _():
            lax.fori_loop(lo, hi, dispatch_far, 0)

    lax.fori_loop(1, 2, dispatch_near, 0)
    dispatch_fars(1, 0, quarter + 1)
    lax.fori_loop(2, half - 1, dispatch_near, 0)
    local = place(0)
    for q in range(tp):
        recv[q, 0] = jnp.dot(
            local, en[:, pl.ds(q * dq, dq)], preferred_element_type=f32
        ).astype(bf16)
    rows_load.wait()
    halo_copy().wait_recv()
    normalize(normed, mg_ref)
    sg_load = load(sg_hbm, w1.at[:, pl.ds(0, sh_width)], 6)
    su_load = load(su_hbm, w1.at[:, pl.ds(sh_width, sh_width)], 7)
    gp_load = load(gp_hbm, w1, 8)
    op_loads = [
        load(op_hbm.at[:, pl.ds(q * dq, dq)], w1.at[pl.ds(q * width, width), :], 9 + q)
        for q in range(tp)
    ]

    def project():
        ip_load.wait()

        def columns(j, _):
            cols = pl.ds(pl.multiple_of(j * bw, bw), bw)
            piece = jnp.dot(normed[...], w1[:, cols], preferred_element_type=f32)
            ext[:, cols] = piece.astype(bf16).astype(f32)
            return 0

        lax.fori_loop(0, width // bw, columns, 0)
        gp_load.start()

        @pl.when(me == 0)
        def _():
            ext[pl.ds(0, halo_rows), :] = jnp.zeros((halo_rows, width), f32)

    def shared():
        sg_load.wait()
        su_load.wait()
        g = jnp.dot(en[...], w1[:, pl.ds(0, sh_width)], preferred_element_type=f32)
        u = jnp.dot(en[...], w1[:, pl.ds(sh_width, sh_width)], preferred_element_type=f32)
        hidden = (jax.nn.silu(g) * u).astype(bf16)
        for one in op_loads:
            one.start()
        sd_load.wait()
        for q in range(tp):
            cols = pl.ds(q * dq, dq)
            piece = jnp.dot(hidden, sd[:, cols], preferred_element_type=f32)
            st[:, :, cols] = piece.reshape(tp, each, dq)
        for k in range(ys):
            pair(st, e_half, ed_s, ed_r, k).start()

    def gate_step():
        gp_load.wait()

        def columns(j, _):
            cols = pl.ds(pl.multiple_of(j * bw, bw), bw)
            piece = jnp.dot(
                normed[pl.ds(halo_rows, rows)], w1[:, cols], preferred_element_type=f32
            )
            gate[:, cols] = jax.nn.gelu(piece)
            return 0

        lax.fori_loop(0, width // bw, columns, 0)
        sg_load.start()
        su_load.start()

    def convolve():
        taps = taps_ref.shape[0]
        base = halo_rows - (taps - 1)
        first = (lax.broadcasted_iota(jnp.int32, (rows, bw), 0) == 0) & (me == 0)
        for b in range(blocks):
            cols = pl.ds(b * bw, bw)
            acc = taps_ref[0:1, cols] * ext[pl.ds(base, rows), cols]
            for k in range(1, taps):
                acc = acc + taps_ref[k : k + 1, cols] * ext[pl.ds(base + k, rows), cols]
            conv = acc.astype(bf16)
            ig = jax.nn.sigmoid(jnp.dot(conv, ig_ref[b], preferred_element_type=f32))
            dg = jax.nn.sigmoid(jnp.dot(conv, dg_ref[b], preferred_element_type=f32))
            ld = -lru_power * dg * softplus_neg(offset_ref[0:1, cols])
            scale = jnp.where(first, 1.0, jnp.sqrt(-expm1_neg(2.0 * ld)))
            a_buf[:, cols] = jnp.exp(ld)
            b_buf[:, cols] = scale * ig * conv.astype(f32)

    def scan():
        row = lax.broadcasted_iota(jnp.int32, (8, width), 0)

        def block(r, carry):
            pc, sc = carry
            at = pl.ds(pl.multiple_of(r * 8, 8), 8)
            a, b = a_buf[at, :], b_buf[at, :]
            for sh in (1, 2, 4):
                keep = row >= sh
                b = jnp.where(keep, b + a * pltpu.roll(b, sh, 0), b)
                a = jnp.where(keep, a * pltpu.roll(a, sh, 0), a)
            b = b + a * sc
            a = a * pc
            a_buf[at, :] = a
            b_buf[at, :] = b
            return a[7:8, :], b[7:8, :]

        pl_last, s_last = lax.fori_loop(
            0, rows // 8, block, (jnp.ones((1, width), f32), jnp.zeros((1, width), f32))
        )
        ends[...] = jnp.where(row == 0, pl_last, s_last)
        for i in range(1, ep):
            end_copy(i).start()

    def carry_in():
        for i in range(1, ep):
            end_copy(i).wait()
        carry = jnp.zeros((1, width), f32)
        for i in range(ep - 1, 0, -1):
            carry = jnp.where(me >= i, got[i, 0:1, :] * carry + got[i, 1:2, :], carry)

        def finish(r, _):
            at = pl.ds(pl.multiple_of(r * 16, 16), 16)
            gated[at, :] = (gate[at, :] * (b_buf[at, :] + a_buf[at, :] * carry)).astype(bf16)
            return 0

        lax.fori_loop(0, rows // 16, finish, 0)

    def project_out():
        for one in op_loads:
            one.wait()
        for q in range(tp):
            piece = jnp.dot(
                gated[...], w1[pl.ds(q * width, width), :], preferred_element_type=f32
            )
            mt[:, :, pl.ds(q * dq, dq)] = piece.reshape(tp, each, dq)
        for k in range(ys):
            pair(mt, m_half, md_s, md_r, k).start()

    def shared_half():
        for k in range(1, ys):
            pair(st, e_half, ed_s, ed_r, k).wait_recv()
            e_out[k] = (e_half[k] + st[up(k)]).astype(bf16)
            ey_copy(k).start()

    def mixer_half():
        for k in range(1, ys):
            pair(mt, m_half, md_s, md_r, k).wait_recv()
            m_out[k] = (m_half[k] + mt[up(k)]).astype(bf16)
            my_copy(k).start()

    def arrive(g):
        for i in blocks_of(g):
            if 2 * g < half:
                for yy in range(ys):
                    z_copy(i, yy).wait_recv()
                for k in range(ys):
                    c_copy(k, i).start()
            else:
                z_copy(i, y).wait_recv()
                for k in range(1, ys):
                    y_copy(k, i).start()
                c_copy(0, i).start()

    def forward(g):
        if 2 * g >= half:
            for i in blocks_of(g):
                for k in range(1, ys):
                    y_copy(k, i).wait_recv()
                    c_copy(k, i).start()

    def feed(g):
        for i in blocks_of(g):
            for k in range(ys):
                c_copy(k, i).wait_recv()
        both = pl.ds(base_of(g), 2)
        gate_sum = up_sum = None
        for q in range(tp):
            x = recv[q, both].reshape(2 * cap, dq)
            span = pl.ds(q * dq, dq)
            g_part = jnp.dot(x, eg[span, :], preferred_element_type=f32)
            u_part = jnp.dot(x, eu[span, :], preferred_element_type=f32)
            gate_sum = g_part if gate_sum is None else gate_sum + g_part
            up_sum = u_part if up_sum is None else up_sum + u_part
        hidden = (jax.nn.silu(gate_sum) * up_sum).astype(bf16)
        hid[t, both] = hidden.reshape(2, cap, hidden.shape[1])
        for k in range(1, ys):
            hy_copy(k, g).start()
        hc_copy(0, g).start()

    def pass_on(g):
        for k in range(1, ys):
            hy_copy(k, g).wait_recv()
            hc_copy(k, g).start()

    def finish(g):
        for k in range(ys):
            hc_copy(k, g).wait_recv()
        both = pl.ds(base_of(g), 2)
        out = None
        for q in range(tp):
            h = hid[q, both].reshape(2 * cap, hid.shape[3])
            part = jnp.dot(h, wd[q], preferred_element_type=f32)
            out = part if out is None else out + part
        out = out.astype(bf16).reshape(2, cap, dq)
        if g == 0:
            back[0] = out[0]
        ret[both] = out
        for i in blocks_of(g):
            b_copy(i).start()

    first_far = groups // 2
    project()
    convolve()
    scan()
    lax.fori_loop(half - 1, half, dispatch_near, 0)
    dispatch_fars(1, quarter + 1, half)
    dispatch_fars(0, 0, half)
    gate_step()
    eg_load.wait()
    eu_load.wait()
    arrive(0)
    arrive(first_far)
    feed(0)
    shared()
    for g in range(1, first_far):
        arrive(g)
        feed(g)
    carry_in()
    project_out()
    wd_load.wait()
    for i in range(1, tp):
        w_copy(i).wait()
    forward(first_far)
    feed(first_far)
    pass_on(0)
    finish(0)
    for g in range(first_far + 1, groups):
        arrive(g)
        pass_on(g - 1)
        finish(g - 1)
        if g == first_far + 1:
            for near in range(1, first_far):
                pass_on(near)
                finish(near)
        forward(g)
        feed(g)
    shared_half()
    mixer_half()
    pass_on(groups - 1)
    finish(groups - 1)

    def combine(lo, count):
        flat = back[pl.ds(lo, count)].reshape(count * cap, dq)
        spot = (lax.broadcasted_iota(jnp.int32, (rows, count * cap), 1) + lo * cap).astype(f32)
        out = None
        for k in range(top):
            pick = (cols_ref[:, k : k + 1] == spot).astype(f32).astype(bf16)
            term = cols_ref[:, top + k : top + k + 1] * jnp.dot(
                pick, flat, preferred_element_type=f32
            )
            out = term if out is None else out + term
        return out.reshape(tp, each, dq)

    for i in range(1, half):
        b_copy(i).wait_recv()
    r_buf[...] = combine(0, half)
    pair(st, e_half, ed_s, ed_r, 0).wait_recv()
    whole = e_half[0] + st[t]
    for k in range(1, ys):
        ey_copy(k).wait_recv()
        whole = whole + e_in[k].astype(f32)
    total[...] = whole
    pair(mt, m_half, md_s, md_r, 0).wait_recv()
    whole = m_half[0] + mt[t]
    for k in range(1, ys):
        my_copy(k).wait_recv()
        whole = whole + m_in[k].astype(f32)
    mo_ref[...] = rms_scale(whole, ms_ref[...]).astype(bf16)
    for i in range(half, ep):
        b_copy(i).wait_recv()
    routed = r_buf[...] + combine(half, half)
    r_out[...] = routed.astype(bf16)
    for k in range(1, ys):
        for core in range(2):
            r_copy(k, core).start()
    r_buf[...] = routed
    r_copy(0, 1).start()
    total[:, mine] = total[:, mine] + r_buf[t]
    r_copy(0, 1).wait()
    near = pl.ds(pl.multiple_of(mate * dq, dq), dq)
    total[:, near] = total[:, near] + r_near[...]
    for k in range(1, ys):
        for core in range(2):
            r_copy(k, core).wait()
            q = down_of(k, lax.rem(c + core, 2))
            cols = pl.ds(pl.multiple_of(q * dq, dq), dq)
            total[:, cols] = total[:, cols] + r_in[q].astype(f32)
    eo_ref[...] = rms_scale(total[...], es_ref[...]).astype(bf16)

    def settle_near(i, _):
        for yy in range(ys):
            z_copy(i, yy).wait_send()
        for k in range(ys):
            c_copy(k, i).wait_send()
        b_copy(i).wait_send()
        return 0

    def settle_far(i, _):
        z_copy(i, y).wait_send()
        for k in range(1, ys):
            y_copy(k, i).wait_send()
        for k in range(ys):
            c_copy(k, i).wait_send()
        b_copy(i).wait_send()
        return 0

    halo_copy().wait_send()
    lax.fori_loop(1, half, settle_near, 0)
    lax.fori_loop(half, ep, settle_far, 0)
    for g in range(groups):
        for k in range(1, ys):
            hy_copy(k, g).wait_send()
        for k in range(ys):
            hc_copy(k, g).wait_send()
    for k in range(ys):
        pair(mt, m_half, md_s, md_r, k).wait_send()
        pair(st, e_half, ed_s, ed_r, k).wait_send()
    for k in range(1, ys):
        my_copy(k).wait_send()
        ey_copy(k).wait_send()


def dma(*shape):
    return pltpu.SemaphoreType.DMA(shape)


def layer(ep, tp, small, large):
    rows, depth = large[0].shape
    width = large[2].shape[1]
    hf, hs = large[5].shape[1], large[8].shape[1]
    top = small[0].shape[0]
    each, ys, dq = rows // tp, tp // 2, depth // tp
    cap = rows * top * 3 // (2 * ep)
    V = pltpu.VMEM
    return pl.pallas_call(
        functools.partial(layer_kernel, ep, tp, top),
        out_shape=[jax.ShapeDtypeStruct((each, depth), bf16)] * 2,
        in_specs=[pl.BlockSpec(memory_space=V)] * len(small)
        + [pl.BlockSpec(memory_space=pl.ANY)] * len(large),
        out_specs=[pl.BlockSpec(memory_space=V)] * 2,
        scratch_shapes=[
            V((ys, ep, cap, dq), bf16),
            V((halo_rows + rows, depth), bf16),
            V((rows, depth), bf16),
            V((ys, each, depth), bf16),
            V((tp, each, dq), bf16),
            V((each, dq), f32),
            V((depth, width), bf16),
            V((depth, hf), bf16),
            V((depth, hf), bf16),
            V((tp, hf, dq), bf16),
            V((hs, depth), bf16),
            V((tp, ep, cap, dq), bf16),
            V((tp, ep, cap, hf), bf16),
            V((ep, cap, dq), bf16),
            V((ep, cap, dq), bf16),
            V((tp, each, depth), f32),
            V((tp, each, depth), f32),
            V((ys, each, depth), f32),
            V((ys, each, depth), f32),
            V((ys, each, depth), bf16),
            V((ys, each, depth), bf16),
            V((ys, each, depth), bf16),
            V((tp, each, dq), f32),
            V((tp, each, dq), bf16),
            V((each, depth), f32),
            V((rows, width), f32),
            V((rows, width), f32),
            V((rows, width), f32),
            V((halo_rows + rows, width), f32),
            V((8, width), f32),
            V((ep, 8, width), f32),
            V((rows, width), bf16),
            V((128, rows), f32),
            V((rows, 128), f32),
            dma(10 + tp), pltpu.SemaphoreType.DMA, pltpu.SemaphoreType.DMA, dma(ep), dma(ep),
            dma(ys, ep), dma(ys, ep),
            dma(ys, ep), dma(ys, ep),
            dma(ys, ep), dma(ys, ep),
            dma(ys, ep // 2), dma(ys, ep // 2),
            dma(ys, ep // 2), dma(ys, ep // 2),
            dma(tp), dma(tp),
            dma(ep), dma(ep),
            dma(ys), dma(ys), dma(ys), dma(ys),
            dma(ys), dma(ys), dma(ys), dma(ys),
            dma(tp), dma(tp),
        ],
        compiler_params=pltpu.CompilerParams(
            collective_id=0, has_side_effects=True, vmem_limit_bytes=67000000
        ),
        name="layer",
    )(*small, *large)


def body(
    mixer_rows, mixer_gain, gate_proj, input_proj, conv_taps, input_gates, decay_gates,
    decay_offset, out_proj, mixer_scale, expert_rows, expert_gain, route_ids, route_weights,
    expert_gate, expert_up, expert_down, shared_gate, shared_up, shared_down, expert_scale,
):
    ep, tp = lax.axis_size("ep"), lax.axis_size("tp")
    gains = [x.reshape(1, -1) for x in (mixer_gain, expert_gain, mixer_scale, expert_scale)]
    small = (
        route_ids.T, route_weights.T, conv_taps, input_gates, decay_gates,
        decay_offset.reshape(1, -1), *gains,
    )
    large = (
        mixer_rows, expert_rows, input_proj, gate_proj, out_proj, expert_gate[0], expert_up[0], expert_down[0],
        shared_gate, shared_up, shared_down,
    )
    return tuple(layer(ep, tp, small, large))


def solution(mesh):
    placed = (
        P("ep", None),
        P(),
        P(None, "tp"),
        P(None, "tp"),
        P(None, "tp"),
        P("tp", None, None),
        P("tp", None, None),
        P("tp"),
        P("tp", None),
        P(),
        P("ep", None),
        P(),
        P("ep", None),
        P("ep", None),
        P("ep", None, "tp"),
        P("ep", None, "tp"),
        P("ep", "tp", None),
        P(None, "tp"),
        P(None, "tp"),
        P("tp", None),
        P(),
    )
    return jax.shard_map(
        body,
        mesh=mesh,
        in_specs=placed,
        out_specs=(P(("ep", "tp"), None), P(("ep", "tp"), None)),
        check_vma=False,
    )
```

```python
import functools

import jax
import jax.numpy as jnp
from jax import lax
from jax.experimental import pallas as pl
from jax.experimental.pallas import tpu as pltpu
from jax.sharding import PartitionSpec as P

eps = 1e-06
lru_power = 8.0
halo_rows = 16
MESH = pl.DeviceIdType.MESH
f32 = jnp.float32
bf16 = jnp.bfloat16


def rms_scale(values, scale):
    floats = values.astype(f32)
    return floats * lax.rsqrt(jnp.mean(floats * floats, axis=-1, keepdims=True) + eps) * scale


def remote(src, dst, send_sem, recv_sem, ep_at, tp_at):
    return pltpu.make_async_remote_copy(
        src_ref=src,
        dst_ref=dst,
        send_sem=send_sem,
        recv_sem=recv_sem,
        device_id=(ep_at, tp_at),
        device_id_type=MESH,
    )


def greet(peers):
    barrier = pltpu.get_barrier_semaphore()
    for ep_at, tp_at in peers:
        pl.semaphore_signal(barrier, inc=1, device_id=(ep_at, tp_at), device_id_type=MESH)
    pl.semaphore_wait(barrier, len(peers))


def expm1_neg(y):
    series = y * (1 + y / 2 * (1 + y / 3 * (1 + y / 4 * (1 + y / 5 * (1 + y / 6 * (1 + y / 7))))))
    return jnp.where(y > -0.35, series, jnp.exp(y) - 1.0)


def softplus_neg(x):
    u = jnp.exp(-jnp.abs(x))
    series = u * (1 - u * (1 / 2 - u * (1 / 3 - u * (1 / 4 - u * (1 / 5 - u / 6)))))
    return jnp.maximum(-x, 0.0) + jnp.where(u < 0.05, series, jnp.log(1.0 + u))


def layer_kernel(
    ep, tp, top,
    ids_ref, weights_ref, taps_ref, ig_ref, dg_ref, offset_ref, mg_ref, xg_ref, ms_ref, es_ref,
    rows_hbm, tokens_hbm, ip_hbm, gp_hbm, op_hbm, eg_hbm, eu_hbm, ed, sg_hbm, su_hbm, sd_hbm,
    mo_ref, eo_ref,
    outq, normed, en, e_out, r_out, r_near,
    w1, eg, eu, wd, sd, recv, hid, ret, back, mt, st, m_half, e_half, m_out, m_in, e_in,
    r_buf, r_in, total, gate, a_buf, b_buf, ext, ends, got, gated, meta, cols_ref,
    load_sem, halo_send, halo_recv, end_send, end_recv,
    z_s, z_r, y_s, y_r, c_s, c_r, hy_s, hy_r, hc_s, hc_r, w_s, w_r, b_s, b_r,
    md_s, md_r, ed_s, ed_r, my_s, my_r, ey_s, ey_r, r_s, r_r,
):
    me, t = lax.axis_index("ep"), lax.axis_index("tp")
    ys = tp // 2
    y, c = t // 2, lax.rem(t, 2)
    mate = y * 2 + 1 - c
    dq = outq.shape[3]
    cap = outq.shape[2]
    rows, width = ext.shape[0] - halo_rows, ext.shape[1]
    each = rows // tp
    blocks, bw = ig_ref.shape[0], ig_ref.shape[1]
    sh_width = sd.shape[0]
    half, quarter = ep // 2, ep // 4
    groups = ep // 2
    inner = lax.rem(me // quarter + 1, 4) // 2

    def at_y(k):
        return lax.rem(y + k, ys)

    def up(k):
        return at_y(k) * 2 + c

    def down_of(k, core):
        return lax.rem(y + ys - k, ys) * 2 + core

    def partner(i):
        out, bit = 0, 1
        while bit < ep:
            out = out + lax.rem(me // bit + i // bit, 2) * bit
            bit *= 2
        return out

    def far(j):
        return half + lax.rem(j + inner * quarter, half)

    def base_of(g):
        return 2 * g if 2 * g < half else far(2 * g - half)

    def blocks_of(g):
        base = base_of(g)
        return [i for i in (base, base + 1) if not (isinstance(i, int) and i == 0)]

    def load(src, dst, at):
        return pltpu.make_async_copy(src, dst, load_sem.at[at])

    tokens_load, rows_load = load(tokens_hbm, en, 0), load(
        rows_hbm, normed.at[pl.ds(halo_rows, rows)], 9 + tp
    )
    tokens_load.start()
    rows_load.start()
    ip_load = load(ip_hbm, w1, 1)
    ip_load.start()

    greet(
        [(lax.rem(me + i, ep), t) for i in range(1, ep)]
        + [(me, lax.rem(t + i, tp)) for i in range(1, tp)]
    )

    def z_copy(i, yy):
        return remote(
            outq.at[yy, i], recv.at[yy * 2 + c, i], z_s.at[yy, i], z_r.at[yy, i], partner(i), t
        )

    def y_copy(k, i):
        return remote(recv.at[t, i], recv.at[t, i], y_s.at[k, i], y_r.at[k, i], me, up(k))

    def c_copy(k, i):
        q = down_of(k, c)
        return remote(recv.at[q, i], recv.at[q, i], c_s.at[k, i], c_r.at[k, i], me, mate)

    def hy_copy(k, g):
        part = hid.at[t, pl.ds(base_of(g), 2)]
        return remote(part, part, hy_s.at[k, g], hy_r.at[k, g], me, up(k))

    def hc_copy(k, g):
        part = hid.at[down_of(k, c), pl.ds(base_of(g), 2)]
        return remote(part, part, hc_s.at[k, g], hc_r.at[k, g], me, mate)

    def w_copy(i):
        q = lax.rem(t + i, tp)
        return remote(
            ed.at[:, pl.ds(pl.multiple_of(q * dq, dq), dq)], wd.at[t],
            w_s.at[i], w_r.at[i], me, q,
        )

    def b_copy(i):
        return remote(ret.at[i], back.at[i], b_s.at[i], b_r.at[i], partner(i), t)

    def halo_copy():
        return remote(
            rows_hbm.at[pl.ds(rows - halo_rows, halo_rows)], normed.at[pl.ds(0, halo_rows)],
            halo_send, halo_recv, lax.rem(me + 1, ep), t,
        )

    def end_copy(i):
        return remote(ends, got.at[i], end_send.at[i], end_recv.at[i], lax.rem(me + i, ep), t)

    def pair(ref, half, s, r, k):
        return remote(ref.at[at_y(k) * 2 + 1 - c], half.at[k], s.at[k], r.at[k], me, mate)

    def my_copy(k):
        return remote(m_out.at[k], m_in.at[k], my_s.at[k], my_r.at[k], me, up(k))

    def ey_copy(k):
        return remote(e_out.at[k], e_in.at[k], ey_s.at[k], ey_r.at[k], me, up(k))

    def r_copy(k, core):
        j, q = 2 * k + core, at_y(k) * 2 + lax.rem(c + core, 2)
        if k == 0:
            return remote(r_buf.at[q], r_near, r_s.at[j], r_r.at[j], me, q)
        return remote(r_out.at[q], r_in.at[t], r_s.at[j], r_r.at[j], me, q)

    def normalize(ref, gain, first):
        def some(r, _):
            at = pl.ds(pl.multiple_of(first + r * 32, 16), 32)
            ref[at, :] = rms_scale(ref[at, :], gain[...]).astype(bf16)
            return 0

        lax.fori_loop(0, rows // 32, some, 0)

    halo_copy().start()
    member = lax.broadcasted_iota(jnp.int32, (ep, rows), 0)
    chosen = [
        (jnp.bitwise_xor(ids_ref[k : k + 1, :], me) == member).astype(f32) for k in range(top)
    ]
    named = chosen[0]
    for k in range(1, top):
        named = named + chosen[k]
    before = lax.broadcasted_iota(jnp.int32, (rows, rows), 0) < lax.broadcasted_iota(
        jnp.int32, (rows, rows), 1
    )
    earlier = jnp.dot(
        named.astype(bf16), before.astype(f32).astype(bf16), preferred_element_type=f32
    )
    spots = earlier + member.astype(f32) * cap
    meta[...] = jnp.zeros_like(meta)
    for k in range(top):
        meta[k : k + 1, :] = jnp.sum(chosen[k] * spots, axis=0, keepdims=True)
        meta[top + k : top + k + 1, :] = weights_ref[k : k + 1, :]
    cols_ref[...] = meta[...].T

    tokens_load.wait()
    for i in range(1, tp):
        w_copy(i).start()
    eg_load, eu_load = load(eg_hbm, eg, 2), load(eu_hbm, eu, 3)
    eg_load.start()
    eu_load.start()
    wd_load = load(ed.at[:, pl.ds(pl.multiple_of(t * dq, dq), dq)], wd.at[t], 4)
    wd_load.start()
    sd_load = load(sd_hbm, sd, 5)
    sd_load.start()
    normalize(en, xg_ref, 0)
    mine = pl.ds(pl.multiple_of(t * dq, dq), dq)

    def place(i):
        spot = (lax.broadcasted_iota(jnp.int32, (cap, rows), 0) + i * cap).astype(f32)
        hot = meta[0:1, :] == spot
        for k in range(1, top):
            hot = hot | (meta[k : k + 1, :] == spot)
        return hot.astype(f32).astype(bf16)

    def dispatch_near(i, _):
        hot = place(i)
        for yy in range(ys):
            part = pl.ds(pl.multiple_of((yy * 2 + c) * dq, dq), dq)
            outq[yy, i] = jnp.dot(hot, en[:, part], preferred_element_type=f32).astype(bf16)
            z_copy(i, yy).start()
        return 0

    def dispatch_far(j, _):
        i = far(j)
        outq[y, i] = jnp.dot(place(i), en[:, mine], preferred_element_type=f32).astype(bf16)
        z_copy(i, y).start()
        return 0

    def dispatch_fars(when, lo, hi):
        @pl.when(inner == when)
        def _():
            lax.fori_loop(lo, hi, dispatch_far, 0)

    def dispatch_nears(when, lo, hi):
        @pl.when(inner == when)
        def _():
            lax.fori_loop(lo, hi, dispatch_near, 0)

    lax.fori_loop(1, quarter, dispatch_near, 0)
    dispatch_fars(1, 0, quarter)
    lax.fori_loop(quarter, half - 1, dispatch_near, 0)
    local = place(0)
    for q in range(tp):
        recv[q, 0] = jnp.dot(
            local, en[:, pl.ds(q * dq, dq)], preferred_element_type=f32
        ).astype(bf16)
    rows_load.wait()
    normalize(normed, mg_ref, halo_rows)
    halo_copy().wait_recv()
    normed[pl.ds(0, halo_rows), :] = rms_scale(
        normed[pl.ds(0, halo_rows), :], mg_ref[...]
    ).astype(bf16)
    sg_load = load(sg_hbm, w1.at[:, pl.ds(0, sh_width)], 6)
    su_load = load(su_hbm, w1.at[:, pl.ds(sh_width, sh_width)], 7)
    gp_load = load(gp_hbm, w1, 8)
    op_loads = [
        load(op_hbm.at[:, pl.ds(q * dq, dq)], w1.at[pl.ds(q * width, width), :], 9 + q)
        for q in range(tp)
    ]

    def project():
        ip_load.wait()

        def columns(j, _):
            cols = pl.ds(pl.multiple_of(j * bw, bw), bw)
            piece = jnp.dot(normed[...], w1[:, cols], preferred_element_type=f32)
            ext[:, cols] = piece.astype(bf16).astype(f32)
            return 0

        lax.fori_loop(0, width // bw, columns, 0)
        gp_load.start()

        @pl.when(me == 0)
        def _():
            ext[pl.ds(0, halo_rows), :] = jnp.zeros((halo_rows, width), f32)

    def shared():
        sg_load.wait()
        su_load.wait()
        g = jnp.dot(en[...], w1[:, pl.ds(0, sh_width)], preferred_element_type=f32)
        u = jnp.dot(en[...], w1[:, pl.ds(sh_width, sh_width)], preferred_element_type=f32)
        hidden = (jax.nn.silu(g) * u).astype(bf16)
        for one in op_loads:
            one.start()
        sd_load.wait()
        for q in range(tp):
            cols = pl.ds(q * dq, dq)
            piece = jnp.dot(hidden, sd[:, cols], preferred_element_type=f32)
            st[:, :, cols] = piece.reshape(tp, each, dq)
        for k in range(ys):
            pair(st, e_half, ed_s, ed_r, k).start()

    def gate_step():
        gp_load.wait()

        def columns(j, _):
            cols = pl.ds(pl.multiple_of(j * bw, bw), bw)
            piece = jnp.dot(
                normed[pl.ds(halo_rows, rows)], w1[:, cols], preferred_element_type=f32
            )
            gate[:, cols] = jax.nn.gelu(piece)
            return 0

        lax.fori_loop(0, width // bw, columns, 0)
        sg_load.start()
        su_load.start()

    def convolve():
        taps = taps_ref.shape[0]
        base = halo_rows - (taps - 1)
        first = (lax.broadcasted_iota(jnp.int32, (rows, bw), 0) == 0) & (me == 0)
        for b in range(blocks):
            cols = pl.ds(b * bw, bw)
            acc = taps_ref[0:1, cols] * ext[pl.ds(base, rows), cols]
            for k in range(1, taps):
                acc = acc + taps_ref[k : k + 1, cols] * ext[pl.ds(base + k, rows), cols]
            conv = acc.astype(bf16)
            ig = jax.nn.sigmoid(jnp.dot(conv, ig_ref[b], preferred_element_type=f32))
            dg = jax.nn.sigmoid(jnp.dot(conv, dg_ref[b], preferred_element_type=f32))
            ld = -lru_power * dg * softplus_neg(offset_ref[0:1, cols])
            scale = jnp.where(first, 1.0, jnp.sqrt(-expm1_neg(2.0 * ld)))
            a_buf[:, cols] = jnp.exp(ld)
            b_buf[:, cols] = scale * ig * conv.astype(f32)

    def scan():
        row = lax.broadcasted_iota(jnp.int32, (8, width), 0)

        def block(r, carry):
            pc, sc = carry
            at = pl.ds(pl.multiple_of(r * 8, 8), 8)
            a, b = a_buf[at, :], b_buf[at, :]
            for sh in (1, 2, 4):
                keep = row >= sh
                b = jnp.where(keep, b + a * pltpu.roll(b, sh, 0), b)
                a = jnp.where(keep, a * pltpu.roll(a, sh, 0), a)
            b = b + a * sc
            a = a * pc
            a_buf[at, :] = a
            b_buf[at, :] = b
            return a[7:8, :], b[7:8, :]

        pl_last, s_last = lax.fori_loop(
            0, rows // 8, block, (jnp.ones((1, width), f32), jnp.zeros((1, width), f32))
        )
        ends[...] = jnp.where(row == 0, pl_last, s_last)
        for i in range(1, ep):
            end_copy(i).start()

    def carry_in():
        for i in range(1, ep):
            end_copy(i).wait()
        carry = jnp.zeros((1, width), f32)
        for i in range(ep - 1, 0, -1):
            carry = jnp.where(me >= i, got[i, 0:1, :] * carry + got[i, 1:2, :], carry)

        def finish(r, _):
            at = pl.ds(pl.multiple_of(r * 16, 16), 16)
            gated[at, :] = (gate[at, :] * (b_buf[at, :] + a_buf[at, :] * carry)).astype(bf16)
            return 0

        lax.fori_loop(0, rows // 16, finish, 0)

    def project_out():
        for one in op_loads:
            one.wait()
        for q in range(tp):
            piece = jnp.dot(
                gated[...], w1[pl.ds(q * width, width), :], preferred_element_type=f32
            )
            mt[:, :, pl.ds(q * dq, dq)] = piece.reshape(tp, each, dq)
        for k in range(ys):
            pair(mt, m_half, md_s, md_r, k).start()

    def shared_half():
        for k in range(1, ys):
            pair(st, e_half, ed_s, ed_r, k).wait_recv()
            e_out[k] = (e_half[k] + st[up(k)]).astype(bf16)
            ey_copy(k).start()

    def mixer_half():
        for k in range(1, ys):
            pair(mt, m_half, md_s, md_r, k).wait_recv()
            m_out[k] = (m_half[k] + mt[up(k)]).astype(bf16)
            my_copy(k).start()

    def arrive(g):
        for i in blocks_of(g):
            if 2 * g < half:
                for yy in range(ys):
                    z_copy(i, yy).wait_recv()
                for k in range(ys):
                    c_copy(k, i).start()
            else:
                z_copy(i, y).wait_recv()
                for k in range(1, ys):
                    y_copy(k, i).start()
                c_copy(0, i).start()

    def forward(g):
        if 2 * g >= half:
            for i in blocks_of(g):
                for k in range(1, ys):
                    y_copy(k, i).wait_recv()
                    c_copy(k, i).start()

    def feed(g):
        for i in blocks_of(g):
            for k in range(ys):
                c_copy(k, i).wait_recv()
        both = pl.ds(base_of(g), 2)
        gate_sum = up_sum = None
        for q in range(tp):
            x = recv[q, both].reshape(2 * cap, dq)
            span = pl.ds(q * dq, dq)
            g_part = jnp.dot(x, eg[span, :], preferred_element_type=f32)
            u_part = jnp.dot(x, eu[span, :], preferred_element_type=f32)
            gate_sum = g_part if gate_sum is None else gate_sum + g_part
            up_sum = u_part if up_sum is None else up_sum + u_part
        hidden = (jax.nn.silu(gate_sum) * up_sum).astype(bf16)
        hid[t, both] = hidden.reshape(2, cap, hidden.shape[1])
        for k in range(1, ys):
            hy_copy(k, g).start()
        hc_copy(0, g).start()

    def pass_on(g):
        for k in range(1, ys):
            hy_copy(k, g).wait_recv()
            hc_copy(k, g).start()

    def finish(g):
        for k in range(ys):
            hc_copy(k, g).wait_recv()
        both = pl.ds(base_of(g), 2)
        out = None
        for q in range(tp):
            h = hid[q, both].reshape(2 * cap, hid.shape[3])
            part = jnp.dot(h, wd[q], preferred_element_type=f32)
            out = part if out is None else out + part
        out = out.astype(bf16).reshape(2, cap, dq)
        if g == 0:
            back[0] = out[0]
        ret[both] = out
        for i in blocks_of(g):
            b_copy(i).start()

    first_far = groups // 2
    project()
    dispatch_fars(1, quarter, half)
    dispatch_nears(0, half - 1, half)
    convolve()
    scan()
    gate_step()
    dispatch_nears(1, half - 1, half)
    dispatch_fars(0, 0, quarter)
    arrive(first_far)
    shared()
    dispatch_fars(0, quarter, half)
    arrive(0)
    eg_load.wait()
    eu_load.wait()
    feed(0)
    forward(first_far)
    feed(first_far)
    for g in range(1, first_far):
        arrive(g)
        feed(g)
    wd_load.wait()
    for i in range(1, tp):
        w_copy(i).wait()
    for g in range(first_far + 1, groups):
        pass_on(g - 1)
        finish(g - 1)
        arrive(g)
        if g == first_far + 1:
            for near in range(first_far):
                pass_on(near)
                finish(near)
        forward(g)
        feed(g)
    shared_half()
    carry_in()
    project_out()
    pass_on(groups - 1)
    finish(groups - 1)
    mixer_half()

    def combine(lo, count):
        flat = back[pl.ds(lo, count)].reshape(count * cap, dq)
        spot = (lax.broadcasted_iota(jnp.int32, (rows, count * cap), 1) + lo * cap).astype(f32)
        out = None
        for k in range(top):
            pick = (cols_ref[:, k : k + 1] == spot).astype(f32).astype(bf16)
            term = cols_ref[:, top + k : top + k + 1] * jnp.dot(
                pick, flat, preferred_element_type=f32
            )
            out = term if out is None else out + term
        return out.reshape(tp, each, dq)

    for i in range(1, half):
        b_copy(i).wait_recv()
    r_buf[...] = combine(0, half)
    pair(st, e_half, ed_s, ed_r, 0).wait_recv()
    whole = e_half[0] + st[t]
    for k in range(1, ys):
        ey_copy(k).wait_recv()
        whole = whole + e_in[k].astype(f32)
    total[...] = whole
    pair(mt, m_half, md_s, md_r, 0).wait_recv()
    whole = m_half[0] + mt[t]
    for k in range(1, ys):
        my_copy(k).wait_recv()
        whole = whole + m_in[k].astype(f32)
    mo_ref[...] = rms_scale(whole, ms_ref[...]).astype(bf16)
    for i in range(half, ep):
        b_copy(i).wait_recv()
    routed = r_buf[...] + combine(half, half)
    r_out[...] = routed.astype(bf16)
    for k in range(1, ys):
        for core in range(2):
            r_copy(k, core).start()
    r_buf[...] = routed
    r_copy(0, 1).start()
    total[:, mine] = total[:, mine] + r_buf[t]
    r_copy(0, 1).wait()
    near = pl.ds(pl.multiple_of(mate * dq, dq), dq)
    total[:, near] = total[:, near] + r_near[...]
    for k in range(1, ys):
        for core in range(2):
            r_copy(k, core).wait()
            q = down_of(k, lax.rem(c + core, 2))
            cols = pl.ds(pl.multiple_of(q * dq, dq), dq)
            total[:, cols] = total[:, cols] + r_in[q].astype(f32)
    eo_ref[...] = rms_scale(total[...], es_ref[...]).astype(bf16)

    def settle_near(i, _):
        for yy in range(ys):
            z_copy(i, yy).wait_send()
        for k in range(ys):
            c_copy(k, i).wait_send()
        b_copy(i).wait_send()
        return 0

    def settle_far(i, _):
        z_copy(i, y).wait_send()
        for k in range(1, ys):
            y_copy(k, i).wait_send()
        for k in range(ys):
            c_copy(k, i).wait_send()
        b_copy(i).wait_send()
        return 0

    halo_copy().wait_send()
    lax.fori_loop(1, half, settle_near, 0)
    lax.fori_loop(half, ep, settle_far, 0)
    for g in range(groups):
        for k in range(1, ys):
            hy_copy(k, g).wait_send()
        for k in range(ys):
            hc_copy(k, g).wait_send()
    for k in range(ys):
        pair(mt, m_half, md_s, md_r, k).wait_send()
        pair(st, e_half, ed_s, ed_r, k).wait_send()
    for k in range(1, ys):
        my_copy(k).wait_send()
        ey_copy(k).wait_send()


def dma(*shape):
    return pltpu.SemaphoreType.DMA(shape)


def layer(ep, tp, small, large):
    rows, depth = large[0].shape
    width = large[2].shape[1]
    hf, hs = large[5].shape[1], large[8].shape[1]
    top = small[0].shape[0]
    each, ys, dq = rows // tp, tp // 2, depth // tp
    cap = rows * top * 3 // (2 * ep)
    V = pltpu.VMEM
    return pl.pallas_call(
        functools.partial(layer_kernel, ep, tp, top),
        out_shape=[jax.ShapeDtypeStruct((each, depth), bf16)] * 2,
        in_specs=[pl.BlockSpec(memory_space=V)] * len(small)
        + [pl.BlockSpec(memory_space=pl.ANY)] * len(large),
        out_specs=[pl.BlockSpec(memory_space=V)] * 2,
        scratch_shapes=[
            V((ys, ep, cap, dq), bf16),
            V((halo_rows + rows, depth), bf16),
            V((rows, depth), bf16),
            V((ys, each, depth), bf16),
            V((tp, each, dq), bf16),
            V((each, dq), f32),
            V((depth, width), bf16),
            V((depth, hf), bf16),
            V((depth, hf), bf16),
            V((tp, hf, dq), bf16),
            V((hs, depth), bf16),
            V((tp, ep, cap, dq), bf16),
            V((tp, ep, cap, hf), bf16),
            V((ep, cap, dq), bf16),
            V((ep, cap, dq), bf16),
            V((tp, each, depth), f32),
            V((tp, each, depth), f32),
            V((ys, each, depth), f32),
            V((ys, each, depth), f32),
            V((ys, each, depth), bf16),
            V((ys, each, depth), bf16),
            V((ys, each, depth), bf16),
            V((tp, each, dq), f32),
            V((tp, each, dq), bf16),
            V((each, depth), f32),
            V((rows, width), f32),
            V((rows, width), f32),
            V((rows, width), f32),
            V((halo_rows + rows, width), f32),
            V((8, width), f32),
            V((ep, 8, width), f32),
            V((rows, width), bf16),
            V((128, rows), f32),
            V((rows, 128), f32),
            dma(10 + tp), pltpu.SemaphoreType.DMA, pltpu.SemaphoreType.DMA, dma(ep), dma(ep),
            dma(ys, ep), dma(ys, ep),
            dma(ys, ep), dma(ys, ep),
            dma(ys, ep), dma(ys, ep),
            dma(ys, ep // 2), dma(ys, ep // 2),
            dma(ys, ep // 2), dma(ys, ep // 2),
            dma(tp), dma(tp),
            dma(ep), dma(ep),
            dma(ys), dma(ys), dma(ys), dma(ys),
            dma(ys), dma(ys), dma(ys), dma(ys),
            dma(tp), dma(tp),
        ],
        compiler_params=pltpu.CompilerParams(
            collective_id=0, has_side_effects=True, vmem_limit_bytes=67000000
        ),
        name="layer",
    )(*small, *large)


def body(
    mixer_rows, mixer_gain, gate_proj, input_proj, conv_taps, input_gates, decay_gates,
    decay_offset, out_proj, mixer_scale, expert_rows, expert_gain, route_ids, route_weights,
    expert_gate, expert_up, expert_down, shared_gate, shared_up, shared_down, expert_scale,
):
    ep, tp = lax.axis_size("ep"), lax.axis_size("tp")
    gains = [x.reshape(1, -1) for x in (mixer_gain, expert_gain, mixer_scale, expert_scale)]
    small = (
        route_ids.T, route_weights.T, conv_taps, input_gates, decay_gates,
        decay_offset.reshape(1, -1), *gains,
    )
    large = (
        mixer_rows, expert_rows, input_proj, gate_proj, out_proj, expert_gate[0], expert_up[0], expert_down[0],
        shared_gate, shared_up, shared_down,
    )
    return tuple(layer(ep, tp, small, large))


def solution(mesh):
    placed = (
        P("ep", None),
        P(),
        P(None, "tp"),
        P(None, "tp"),
        P(None, "tp"),
        P("tp", None, None),
        P("tp", None, None),
        P("tp"),
        P("tp", None),
        P(),
        P("ep", None),
        P(),
        P("ep", None),
        P("ep", None),
        P("ep", None, "tp"),
        P("ep", None, "tp"),
        P("ep", "tp", None),
        P(None, "tp"),
        P(None, "tp"),
        P("tp", None),
        P(),
    )
    return jax.shard_map(
        body,
        mesh=mesh,
        in_specs=placed,
        out_specs=(P(("ep", "tp"), None), P(("ep", "tp"), None)),
        check_vma=False,
    )
```

```python
import functools

import jax
import jax.numpy as jnp
from jax import lax
from jax.experimental import pallas as pl
from jax.experimental.pallas import tpu as pltpu
from jax.sharding import PartitionSpec as P

eps = 1e-06
lru_power = 8.0
halo_rows = 16
MESH = pl.DeviceIdType.MESH
f32 = jnp.float32
bf16 = jnp.bfloat16


def rms_scale(values, scale):
    floats = values.astype(f32)
    return floats * lax.rsqrt(jnp.mean(floats * floats, axis=-1, keepdims=True) + eps) * scale


def remote(src, dst, send_sem, recv_sem, ep_at, tp_at):
    return pltpu.make_async_remote_copy(
        src_ref=src,
        dst_ref=dst,
        send_sem=send_sem,
        recv_sem=recv_sem,
        device_id=(ep_at, tp_at),
        device_id_type=MESH,
    )


def greet(peers):
    barrier = pltpu.get_barrier_semaphore()
    for ep_at, tp_at in peers:
        pl.semaphore_signal(barrier, inc=1, device_id=(ep_at, tp_at), device_id_type=MESH)


def meet(count):
    pl.semaphore_wait(pltpu.get_barrier_semaphore(), count)


def expm1_neg(y):
    series = y * (1 + y / 2 * (1 + y / 3 * (1 + y / 4 * (1 + y / 5 * (1 + y / 6 * (1 + y / 7))))))
    return jnp.where(y > -0.35, series, jnp.exp(y) - 1.0)


def softplus_neg(x):
    u = jnp.exp(-jnp.abs(x))
    series = u * (1 - u * (1 / 2 - u * (1 / 3 - u * (1 / 4 - u * (1 / 5 - u / 6)))))
    return jnp.maximum(-x, 0.0) + jnp.where(u < 0.05, series, jnp.log(1.0 + u))


def layer_kernel(
    ep, tp, top,
    count, *refs,
):
    small_hbm, large, small = refs[:count], refs[count:-count], refs[-count:]
    layer_body(ep, tp, top, small_hbm, small, *large)


def layer_body(
    ep, tp, top, small_hbm, small,
    rows_hbm, tokens_hbm, ip_hbm, gp_hbm, op_hbm, eg_hbm, eu_hbm, ed, sg_hbm, su_hbm, sd_hbm,
    mo_hbm, eo_hbm,
    outq, normed, en, e_out, r_out, r_near,
    w1, eg, eu, wd, sd, recv, hid, ret, back, mt, st, m_half, e_half, m_out, m_in, e_in,
    r_buf, r_in, total, gate, a_buf, b_buf, ext, ends, got, gated, meta, cols_ref, mo_ref, eo_ref,
    load_sem, small_sem, out_sem, halo_send, halo_recv, end_send, end_recv,
    z_s, z_r, y_s, y_r, c_s, c_r, hy_s, hy_r, hc_s, hc_r, w_s, w_r, b_s, b_r,
    md_s, md_r, ed_s, ed_r, my_s, my_r, ey_s, ey_r, r_s, r_r, l_s, l_r,
):
    ids_ref, weights_ref, xg_ref, taps_ref, ig_ref, dg_ref, offset_ref, mg_ref, ms_ref, es_ref = small
    me, t = lax.axis_index("ep"), lax.axis_index("tp")
    ys = tp // 2
    y, c = t // 2, lax.rem(t, 2)
    mate = y * 2 + 1 - c
    dq = outq.shape[3]
    cap = outq.shape[2]
    rows, width = ext.shape[0] - halo_rows, ext.shape[1]
    each = rows // tp
    blocks, bw = ig_ref.shape[0], ig_ref.shape[1]
    sh_width = sd.shape[0]
    half, quarter = ep // 2, ep // 4
    sizes = [2] * quarter + [1] * half
    groups, first_far = quarter + half, quarter
    inner = lax.rem(me // quarter + 1, 4) // 2

    def at_y(k):
        return lax.rem(y + k, ys)

    def up(k):
        return at_y(k) * 2 + c

    def down_of(k, core):
        return lax.rem(y + ys - k, ys) * 2 + core

    def partner(i):
        out, bit = 0, 1
        while bit < ep:
            out = out + lax.rem(me // bit + i // bit, 2) * bit
            bit *= 2
        return out

    def far(j):
        return half + lax.rem(j + inner * quarter, half)

    def base_of(g):
        start = sum(sizes[:g])
        return start if start < half else far(start - half)

    def span_of(g):
        return pl.ds(base_of(g), sizes[g])

    def blocks_of(g):
        return [base_of(g) + n for n in range(sizes[g]) if g + n > 0]

    def load(src, dst, at):
        return pltpu.make_async_copy(src, dst, load_sem.at[at])

    peers = [(lax.rem(me + i, ep), t) for i in range(1, ep)] + [
        (me, lax.rem(t + i, tp)) for i in range(1, tp)
    ]
    greet(peers)
    small_loads = [
        pltpu.make_async_copy(src, dst, small_sem.at[n])
        for n, (src, dst) in enumerate(zip(small_hbm, small))
    ]
    tokens_load, rows_load = load(tokens_hbm, en, 0), load(
        rows_hbm, normed.at[pl.ds(halo_rows, rows)], 9 + tp
    )
    ip_load = load(ip_hbm, w1, 1)
    tokens_load.start()
    for one in small_loads[:3]:
        one.start()

    def z_copy(i, yy, near):
        n = yy * half + i if near else ys * half - half + i
        return remote(outq.at[yy, i], recv.at[yy * 2 + c, i], z_s.at[n], z_r.at[n], partner(i), t)

    def y_copy(k, i):
        n = i - half
        part = recv.at[t, i]
        return remote(part, part, y_s.at[k - 1, n], y_r.at[k - 1, n], me, up(k))

    def c_copy(k, i):
        q = down_of(k, c)
        return remote(recv.at[q, i], recv.at[q, i], c_s.at[k, i - 1], c_r.at[k, i - 1], me, mate)

    def hy_copy(k, g):
        part = hid.at[t, span_of(g)]
        return remote(part, part, hy_s.at[k - 1, g], hy_r.at[k - 1, g], me, up(k))

    def hc_copy(k, g):
        part = hid.at[down_of(k, c), span_of(g)]
        return remote(part, part, hc_s.at[k, g], hc_r.at[k, g], me, mate)

    def w_copy(i):
        q = lax.rem(t + i, tp)
        return remote(
            ed.at[:, pl.ds(pl.multiple_of(q * dq, dq), dq)], wd.at[t],
            w_s.at[i - 1], w_r.at[i - 1], me, q,
        )

    def b_copy(i):
        return remote(ret.at[i], back.at[i], b_s.at[i - 1], b_r.at[i - 1], partner(i), t)

    def halo_copy():
        return remote(
            rows_hbm.at[pl.ds(rows - halo_rows, halo_rows)], normed.at[pl.ds(0, halo_rows)],
            halo_send, halo_recv, lax.rem(me + 1, ep), t,
        )

    def end_copy(i):
        n, to = i - 1, lax.rem(me + i, ep)
        return remote(ends, got.at[i], end_send.at[n], end_recv.at[n], to, t)

    def pair(ref, half, s, r, k):
        return remote(ref.at[at_y(k) * 2 + 1 - c], half.at[k], s.at[k], r.at[k], me, mate)

    def my_copy(k):
        return remote(m_out.at[k], m_in.at[k], my_s.at[k - 1], my_r.at[k - 1], me, up(k))

    def ey_copy(k, j):
        s, r = ey_s.at[k - 1, j - 1], ey_r.at[k - 1, j - 1]
        return remote(e_out.at[k, j], e_in.at[k, j], s, r, me, up(k))

    def r_copy(k):
        return remote(r_buf.at[at_y(k) * 2 + 1 - c], r_near.at[k], r_s.at[k], r_r.at[k], me, mate)

    def late_copy(k, j):
        s, r = l_s.at[k - 1, j], l_r.at[k - 1, j]
        return remote(r_out.at[k, j], r_in.at[k, j], s, r, me, up(k))

    def of_chip(yy):
        return pl.ds(pl.multiple_of(yy * 2 * dq, dq), 2 * dq)

    def of_core(yy, core):
        return pl.ds(pl.multiple_of((yy * 2 + core) * dq, dq), dq)

    def normalize(ref, gain, first):
        def some(r, _):
            at = pl.ds(pl.multiple_of(first + r * 32, 16), 32)
            ref[at, :] = rms_scale(ref[at, :], gain[...]).astype(bf16)
            return 0

        lax.fori_loop(0, rows // 32, some, 0)

    for one in small_loads[:3]:
        one.wait()
    member = lax.broadcasted_iota(jnp.int32, (ep, rows), 0)
    chosen = [
        (jnp.bitwise_xor(ids_ref[k : k + 1, :], me) == member).astype(f32) for k in range(top)
    ]
    named = chosen[0]
    for k in range(1, top):
        named = named + chosen[k]
    before = lax.broadcasted_iota(jnp.int32, (rows, rows), 0) < lax.broadcasted_iota(
        jnp.int32, (rows, rows), 1
    )
    earlier = jnp.dot(
        named.astype(bf16), before.astype(f32).astype(bf16), preferred_element_type=f32
    )
    spots = earlier + member.astype(f32) * cap
    meta[...] = jnp.zeros_like(meta)
    for k in range(top):
        meta[k : k + 1, :] = jnp.sum(chosen[k] * spots, axis=0, keepdims=True)
        meta[top + k : top + k + 1, :] = weights_ref[k : k + 1, :]
    cols_ref[...] = meta[...].T

    tokens_load.wait()
    rows_load.start()
    for one in small_loads[3:]:
        one.start()
    ip_load.start()
    normalize(en, xg_ref, 0)
    meet(len(peers))
    halo_copy().start()
    for i in range(1, tp):
        w_copy(i).start()
    eg_load, eu_load = load(eg_hbm, eg, 2), load(eu_hbm, eu, 3)
    eg_load.start()
    eu_load.start()
    wd_load = load(ed.at[:, pl.ds(pl.multiple_of(t * dq, dq), dq)], wd.at[t], 4)
    wd_load.start()
    sd_load = load(sd_hbm, sd, 5)
    sd_load.start()
    mine = pl.ds(pl.multiple_of(t * dq, dq), dq)

    def place(i):
        spot = (lax.broadcasted_iota(jnp.int32, (cap, rows), 0) + i * cap).astype(f32)
        hot = meta[0:1, :] == spot
        for k in range(1, top):
            hot = hot | (meta[k : k + 1, :] == spot)
        return hot.astype(f32).astype(bf16)

    def dispatch_near(i, _):
        hot = place(i)
        for yy in range(ys):
            part = pl.ds(pl.multiple_of((yy * 2 + c) * dq, dq), dq)
            outq[yy, i] = jnp.dot(hot, en[:, part], preferred_element_type=f32).astype(bf16)
            z_copy(i, yy, True).start()
        return 0

    def dispatch_far(j, _):
        i = far(j)
        outq[y, i] = jnp.dot(place(i), en[:, mine], preferred_element_type=f32).astype(bf16)
        z_copy(i, y, False).start()
        return 0

    def dispatch_fars(when, lo, hi):
        @pl.when(inner == when)
        def _():
            lax.fori_loop(lo, hi, dispatch_far, 0)

    def dispatch_nears(when, lo, hi):
        @pl.when(inner == when)
        def _():
            lax.fori_loop(lo, hi, dispatch_near, 0)

    lax.fori_loop(1, quarter, dispatch_near, 0)
    dispatch_fars(1, 0, quarter)
    lax.fori_loop(quarter, half - 1, dispatch_near, 0)
    local = place(0)
    for q in range(tp):
        recv[q, 0] = jnp.dot(
            local, en[:, pl.ds(q * dq, dq)], preferred_element_type=f32
        ).astype(bf16)
    dispatch_fars(1, quarter, half - 1)
    for one in small_loads[3:]:
        one.wait()
    rows_load.wait()
    normalize(normed, mg_ref, halo_rows)
    halo_copy().wait_recv()
    normed[pl.ds(0, halo_rows), :] = rms_scale(
        normed[pl.ds(0, halo_rows), :], mg_ref[...]
    ).astype(bf16)
    sg_load = load(sg_hbm, w1.at[:, pl.ds(0, sh_width)], 6)
    su_load = load(su_hbm, w1.at[:, pl.ds(sh_width, sh_width)], 7)
    gp_load = load(gp_hbm, w1, 8)
    op_loads = [
        load(op_hbm.at[:, pl.ds(q * dq, dq)], w1.at[pl.ds(q * width, width), :], 9 + q)
        for q in range(tp)
    ]

    def project():
        ip_load.wait()

        def columns(j, _):
            cols = pl.ds(pl.multiple_of(j * bw, bw), bw)
            piece = jnp.dot(normed[...], w1[:, cols], preferred_element_type=f32)
            ext[:, cols] = piece.astype(bf16).astype(f32)
            return 0

        lax.fori_loop(0, width // bw, columns, 0)
        gp_load.start()

        @pl.when(me == 0)
        def _():
            ext[pl.ds(0, halo_rows), :] = jnp.zeros((halo_rows, width), f32)

    def shared():
        sg_load.wait()
        su_load.wait()
        g = jnp.dot(en[...], w1[:, pl.ds(0, sh_width)], preferred_element_type=f32)
        u = jnp.dot(en[...], w1[:, pl.ds(sh_width, sh_width)], preferred_element_type=f32)
        hidden = (jax.nn.silu(g) * u).astype(bf16)
        for one in op_loads:
            one.start()
        sd_load.wait()
        for q in range(tp):
            cols = pl.ds(q * dq, dq)
            piece = jnp.dot(hidden, sd[:, cols], preferred_element_type=f32)
            st[:, :, cols] = piece.reshape(tp, each, dq)
        for k in range(ys):
            pair(st, e_half, ed_s, ed_r, k).start()

    def gate_step():
        gp_load.wait()

        def columns(j, _):
            cols = pl.ds(pl.multiple_of(j * bw, bw), bw)
            piece = jnp.dot(
                normed[pl.ds(halo_rows, rows)], w1[:, cols], preferred_element_type=f32
            )
            gate[:, cols] = jax.nn.gelu(piece)
            return 0

        lax.fori_loop(0, width // bw, columns, 0)
        sg_load.start()
        su_load.start()

    def convolve():
        taps = taps_ref.shape[0]
        base = halo_rows - (taps - 1)
        first = (lax.broadcasted_iota(jnp.int32, (rows, bw), 0) == 0) & (me == 0)
        for b in range(blocks):
            cols = pl.ds(b * bw, bw)
            acc = taps_ref[0:1, cols] * ext[pl.ds(base, rows), cols]
            for k in range(1, taps):
                acc = acc + taps_ref[k : k + 1, cols] * ext[pl.ds(base + k, rows), cols]
            conv = acc.astype(bf16)
            ig = jax.nn.sigmoid(jnp.dot(conv, ig_ref[b], preferred_element_type=f32))
            dg = jax.nn.sigmoid(jnp.dot(conv, dg_ref[b], preferred_element_type=f32))
            ld = -lru_power * dg * softplus_neg(offset_ref[0:1, cols])
            scale = jnp.where(first, 1.0, jnp.sqrt(-expm1_neg(2.0 * ld)))
            a_buf[:, cols] = jnp.exp(ld)
            b_buf[:, cols] = scale * ig * conv.astype(f32)

    def scan():
        row = lax.broadcasted_iota(jnp.int32, (8, width), 0)

        def block(r, carry):
            pc, sc = carry
            at = pl.ds(pl.multiple_of(r * 8, 8), 8)
            a, b = a_buf[at, :], b_buf[at, :]
            for sh in (1, 2, 4):
                keep = row >= sh
                b = jnp.where(keep, b + a * pltpu.roll(b, sh, 0), b)
                a = jnp.where(keep, a * pltpu.roll(a, sh, 0), a)
            b = b + a * sc
            a = a * pc
            a_buf[at, :] = a
            b_buf[at, :] = b
            return a[7:8, :], b[7:8, :]

        pl_last, s_last = lax.fori_loop(
            0, rows // 8, block, (jnp.ones((1, width), f32), jnp.zeros((1, width), f32))
        )
        ends[...] = jnp.where(row == 0, pl_last, s_last)
        for i in range(1, ep):
            end_copy(i).start()

    def carry_in():
        for i in range(1, ep):
            end_copy(i).wait()
        carry = jnp.zeros((1, width), f32)
        for i in range(ep - 1, 0, -1):
            carry = jnp.where(me >= i, got[i, 0:1, :] * carry + got[i, 1:2, :], carry)

        def finish(r, _):
            at = pl.ds(pl.multiple_of(r * 16, 16), 16)
            gated[at, :] = (gate[at, :] * (b_buf[at, :] + a_buf[at, :] * carry)).astype(bf16)
            return 0

        lax.fori_loop(0, rows // 16, finish, 0)

    def project_out():
        for one in op_loads:
            one.wait()
        for q in range(tp):
            piece = jnp.dot(
                gated[...], w1[pl.ds(q * width, width), :], preferred_element_type=f32
            )
            mt[:, :, pl.ds(q * dq, dq)] = piece.reshape(tp, each, dq)

    def shared_half():
        for k in range(1, ys):
            pair(st, e_half, ed_s, ed_r, k).wait_recv()
            for j in range(1, ys):
                cols = of_chip(at_y(j))
                e_out[k, j] = (e_half[k, :, cols] + st[up(k), :, cols]).astype(bf16)
                ey_copy(k, j).start()

    def mixer_half():
        for k in range(1, ys):
            pair(mt, m_half, md_s, md_r, k).wait_recv()
            m_out[k] = (m_half[k] + mt[up(k)]).astype(bf16)
            my_copy(k).start()

    def arrive(g):
        for i in blocks_of(g):
            if g < first_far:
                for yy in range(ys):
                    z_copy(i, yy, True).wait_recv()
                for k in range(ys):
                    c_copy(k, i).start()
            else:
                z_copy(i, y, False).wait_recv()
                for k in range(1, ys):
                    y_copy(k, i).start()
                c_copy(0, i).start()

    def forward(g):
        if g >= first_far:
            for i in blocks_of(g):
                for k in range(1, ys):
                    y_copy(k, i).wait_recv()
                    c_copy(k, i).start()

    def feed(g):
        for i in blocks_of(g):
            for k in range(ys):
                c_copy(k, i).wait_recv()
        both = span_of(g)
        gate_sum = up_sum = None
        for q in range(tp):
            x = recv[q, both].reshape(sizes[g] * cap, dq)
            span = pl.ds(q * dq, dq)
            g_part = jnp.dot(x, eg[span, :], preferred_element_type=f32)
            u_part = jnp.dot(x, eu[span, :], preferred_element_type=f32)
            gate_sum = g_part if gate_sum is None else gate_sum + g_part
            up_sum = u_part if up_sum is None else up_sum + u_part
        hidden = (jax.nn.silu(gate_sum) * up_sum).astype(bf16)
        hid[t, both] = hidden.reshape(sizes[g], cap, hidden.shape[1])
        for k in range(1, ys):
            hy_copy(k, g).start()
        hc_copy(0, g).start()

    def pass_on(g):
        for k in range(1, ys):
            hy_copy(k, g).wait_recv()
            hc_copy(k, g).start()

    def finish(g):
        for k in range(ys):
            hc_copy(k, g).wait_recv()
        both = span_of(g)
        out = None
        for q in range(tp):
            h = hid[q, both].reshape(sizes[g] * cap, hid.shape[3])
            part = jnp.dot(h, wd[q], preferred_element_type=f32)
            out = part if out is None else out + part
        out = out.astype(bf16).reshape(sizes[g], cap, dq)
        if g == 0:
            back[0] = out[0]
        ret[both] = out
        for i in blocks_of(g):
            b_copy(i).start()

    project()
    dispatch_fars(1, half - 1, half)
    dispatch_nears(0, half - 1, half)
    convolve()
    scan()
    gate_step()
    dispatch_nears(1, half - 1, half)
    dispatch_fars(0, 0, quarter)
    arrive(first_far)
    shared()
    dispatch_fars(0, quarter, half)
    arrive(first_far + 1)
    arrive(0)
    eg_load.wait()
    eu_load.wait()
    feed(0)
    wd_load.wait()
    for g in (first_far, first_far + 1):
        forward(g)
        feed(g)
    for i in range(1, tp):
        w_copy(i).wait()
    for g in (first_far, first_far + 1):
        pass_on(g)
        finish(g)
    for g in range(1, first_far):
        arrive(g)
        feed(g)
    last = groups - 2
    for g in range(first_far + 2, last):
        arrive(g)
        forward(g)
        feed(g)
        pass_on(g)
        finish(g)
    arrive(last)
    pass_on(0)
    finish(0)
    arrive(last + 1)
    for near in range(1, first_far):
        pass_on(near)
        finish(near)
    forward(last)
    feed(last)
    forward(last + 1)
    feed(last + 1)
    pass_on(last)
    finish(last)
    shared_half()
    carry_in()
    project_out()
    pass_on(last + 1)
    for k in range(ys):
        pair(mt, m_half, md_s, md_r, k).start()
    finish(last + 1)
    mixer_half()

    def combine(lo, count):
        flat = back[pl.ds(lo, count)].reshape(count * cap, dq)
        spot = (lax.broadcasted_iota(jnp.int32, (rows, count * cap), 1) + lo * cap).astype(f32)
        out = None
        for k in range(top):
            pick = (cols_ref[:, k : k + 1] == spot).astype(f32).astype(bf16)
            term = cols_ref[:, top + k : top + k + 1] * jnp.dot(
                pick, flat, preferred_element_type=f32
            )
            out = term if out is None else out + term
        return out.reshape(tp, each, dq)

    for i in range(1, half):
        b_copy(i).wait_recv()
    r_buf[...] = combine(0, half)
    pair(st, e_half, ed_s, ed_r, 0).wait_recv()
    total[...] = e_half[0] + st[t]
    for k in range(1, ys):
        for j in range(1, ys):
            ey_copy(k, j).wait_recv()
            cols = of_chip(lax.rem(y + ys - k + j, ys))
            total[:, cols] = total[:, cols] + e_in[k, j].astype(f32)
    pair(mt, m_half, md_s, md_r, 0).wait_recv()
    whole = m_half[0] + mt[t]
    for k in range(1, ys):
        my_copy(k).wait_recv()
        whole = whole + m_in[k].astype(f32)
    mo_ref[...] = rms_scale(whole, ms_ref[...]).astype(bf16)
    mo_store = pltpu.make_async_copy(mo_ref, mo_hbm, out_sem.at[0])
    mo_store.start()
    for i in range(half, ep):
        b_copy(i).wait_recv()
    r_buf[...] = r_buf[...] + combine(half, half)
    for k in range(ys):
        r_copy(k).start()
    near = of_core(y, 1 - c)
    for k in range(1, ys):
        r_out[k, 0] = (e_half[k, :, mine] + st[up(k), :, mine] + r_buf[up(k)]).astype(bf16)
        late_copy(k, 0).start()
    for k in range(1, ys):
        r_copy(k).wait_recv()
        r_out[k, 1] = (e_half[k, :, near] + st[up(k), :, near] + r_near[k]).astype(bf16)
        late_copy(k, 1).start()
    total[:, mine] = total[:, mine] + r_buf[t]
    r_copy(0).wait_recv()
    total[:, near] = total[:, near] + r_near[0]
    for k in range(1, ys):
        for j in range(2):
            late_copy(k, j).wait_recv()
            cols = of_core(lax.rem(y + ys - k, ys), lax.rem(c + j, 2))
            total[:, cols] = total[:, cols] + r_in[k, j].astype(f32)
    eo_ref[...] = rms_scale(total[...], es_ref[...]).astype(bf16)
    eo_store = pltpu.make_async_copy(eo_ref, eo_hbm, out_sem.at[1])
    eo_store.start()

    def settle_near(i, _):
        for yy in range(ys):
            z_copy(i, yy, True).wait_send()
        for k in range(ys):
            c_copy(k, i).wait_send()
        b_copy(i).wait_send()
        return 0

    def settle_far(i, _):
        z_copy(i, y, False).wait_send()
        for k in range(1, ys):
            y_copy(k, i).wait_send()
        for k in range(ys):
            c_copy(k, i).wait_send()
        b_copy(i).wait_send()
        return 0

    halo_copy().wait_send()
    lax.fori_loop(1, half, settle_near, 0)
    lax.fori_loop(half, ep, settle_far, 0)
    for g in range(groups):
        for k in range(1, ys):
            hy_copy(k, g).wait_send()
        for k in range(ys):
            hc_copy(k, g).wait_send()
    for k in range(ys):
        pair(mt, m_half, md_s, md_r, k).wait_send()
        pair(st, e_half, ed_s, ed_r, k).wait_send()
    for k in range(ys):
        r_copy(k).wait_send()
    for k in range(1, ys):
        my_copy(k).wait_send()
        for j in range(1, ys):
            ey_copy(k, j).wait_send()
        for j in range(2):
            late_copy(k, j).wait_send()
    mo_store.wait()
    eo_store.wait()


def dma(*shape):
    return pltpu.SemaphoreType.DMA(shape)


def layer(ep, tp, small, large):
    rows, depth = large[0].shape
    width = large[2].shape[1]
    hf, hs = large[5].shape[1], large[8].shape[1]
    top = small[0].shape[0]
    each, ys, dq = rows // tp, tp // 2, depth // tp
    groups = ep // 4 + ep // 2
    cap = rows * top * 3 // (2 * ep)
    V = pltpu.VMEM
    return pl.pallas_call(
        functools.partial(layer_kernel, ep, tp, top, len(small)),
        out_shape=[jax.ShapeDtypeStruct((each, depth), bf16)] * 2,
        in_specs=[pl.BlockSpec(memory_space=pl.ANY)] * (len(small) + len(large)),
        out_specs=[pl.BlockSpec(memory_space=pl.ANY)] * 2,
        scratch_shapes=[
            V((ys, ep, cap, dq), bf16),
            V((halo_rows + rows, depth), bf16),
            V((rows, depth), bf16),
            V((ys, ys, each, 2 * dq), bf16),
            V((ys, 2, each, dq), bf16),
            V((ys, each, dq), f32),
            V((depth, width), bf16),
            V((depth, hf), bf16),
            V((depth, hf), bf16),
            V((tp, hf, dq), bf16),
            V((hs, depth), bf16),
            V((tp, ep, cap, dq), bf16),
            V((tp, ep, cap, hf), bf16),
            V((ep, cap, dq), bf16),
            V((ep, cap, dq), bf16),
            V((tp, each, depth), f32),
            V((tp, each, depth), f32),
            V((ys, each, depth), f32),
            V((ys, each, depth), f32),
            V((ys, each, depth), bf16),
            V((ys, each, depth), bf16),
            V((ys, ys, each, 2 * dq), bf16),
            V((tp, each, dq), f32),
            V((ys, 2, each, dq), bf16),
            V((each, depth), f32),
            V((rows, width), f32),
            V((rows, width), f32),
            V((rows, width), f32),
            V((halo_rows + rows, width), f32),
            V((8, width), f32),
            V((ep, 8, width), f32),
            V((rows, width), bf16),
            V((128, rows), f32),
            V((rows, 128), f32),
            V((each, depth), bf16),
            V((each, depth), bf16),
            dma(10 + tp), dma(len(small)), dma(2), pltpu.SemaphoreType.DMA, pltpu.SemaphoreType.DMA,
            dma(ep - 1), dma(ep - 1),
            dma((ys + 1) * ep // 2), dma((ys + 1) * ep // 2),
            dma(ys - 1, ep // 2), dma(ys - 1, ep // 2),
            dma(ys, ep - 1), dma(ys, ep - 1),
            dma(ys - 1, groups), dma(ys - 1, groups),
            dma(ys, groups), dma(ys, groups),
            dma(tp - 1), dma(tp - 1),
            dma(ep - 1), dma(ep - 1),
            dma(ys), dma(ys), dma(ys), dma(ys),
            dma(ys - 1), dma(ys - 1), dma(ys - 1, ys - 1), dma(ys - 1, ys - 1),
            dma(ys), dma(ys), dma(ys - 1, 2), dma(ys - 1, 2),
        ]
        + [V(x.shape, x.dtype) for x in small],
        compiler_params=pltpu.CompilerParams(
            collective_id=0, has_side_effects=True, vmem_limit_bytes=67000000
        ),
        name="layer",
    )(*small, *large)


def publish_kernel(mixer, expert, mixer_out, expert_out):
    mixer_out[...] = mixer[...]
    expert_out[...] = expert[...]


def publish(mixer, expert):
    return pl.pallas_call(
        publish_kernel,
        out_shape=[jax.ShapeDtypeStruct(x.shape, x.dtype) for x in (mixer, expert)],
        in_specs=[pl.BlockSpec(memory_space=pltpu.VMEM)] * 2,
        out_specs=[pl.BlockSpec(memory_space=pltpu.VMEM)] * 2,
        name="publish",
    )(mixer, expert)


def body(
    mixer_rows, mixer_gain, gate_proj, input_proj, conv_taps, input_gates, decay_gates,
    decay_offset, out_proj, mixer_scale, expert_rows, expert_gain, route_ids, route_weights,
    expert_gate, expert_up, expert_down, shared_gate, shared_up, shared_down, expert_scale,
):
    ep, tp = lax.axis_size("ep"), lax.axis_size("tp")
    gains = [x.reshape(1, -1) for x in (mixer_gain, expert_gain, mixer_scale, expert_scale)]
    small = (
        route_ids.T, route_weights.T, gains[1], conv_taps, input_gates, decay_gates,
        decay_offset.reshape(1, -1), gains[0], gains[2], gains[3],
    )
    large = (
        mixer_rows, expert_rows, input_proj, gate_proj, out_proj, expert_gate[0], expert_up[0], expert_down[0],
        shared_gate, shared_up, shared_down,
    )
    return tuple(publish(*layer(ep, tp, small, large)))


def solution(mesh):
    placed = (
        P("ep", None),
        P(),
        P(None, "tp"),
        P(None, "tp"),
        P(None, "tp"),
        P("tp", None, None),
        P("tp", None, None),
        P("tp"),
        P("tp", None),
        P(),
        P("ep", None),
        P(),
        P("ep", None),
        P("ep", None),
        P("ep", None, "tp"),
        P("ep", None, "tp"),
        P("ep", "tp", None),
        P(None, "tp"),
        P(None, "tp"),
        P("tp", None),
        P(),
    )
    return jax.shard_map(
        body,
        mesh=mesh,
        in_specs=placed,
        out_specs=(P(("ep", "tp"), None), P(("ep", "tp"), None)),
        check_vma=False,
    )
```

```python
import functools

import jax
import jax.numpy as jnp
from jax import lax
from jax.experimental import pallas as pl
from jax.experimental.pallas import tpu as pltpu
from jax.sharding import PartitionSpec as P

eps = 1e-06
lru_power = 8.0
halo_rows = 16
MESH = pl.DeviceIdType.MESH
f32 = jnp.float32
bf16 = jnp.bfloat16


def rms_scale(values, scale):
    floats = values.astype(f32)
    return floats * lax.rsqrt(jnp.mean(floats * floats, axis=-1, keepdims=True) + eps) * scale


def remote(src, dst, send_sem, recv_sem, ep_at, tp_at):
    return pltpu.make_async_remote_copy(
        src_ref=src,
        dst_ref=dst,
        send_sem=send_sem,
        recv_sem=recv_sem,
        device_id=(ep_at, tp_at),
        device_id_type=MESH,
    )


def greet(peers):
    barrier = pltpu.get_barrier_semaphore()
    for ep_at, tp_at in peers:
        pl.semaphore_signal(barrier, inc=1, device_id=(ep_at, tp_at), device_id_type=MESH)


def meet(count):
    pl.semaphore_wait(pltpu.get_barrier_semaphore(), count)


def expm1_neg(y):
    series = y * (1 + y / 2 * (1 + y / 3 * (1 + y / 4 * (1 + y / 5 * (1 + y / 6 * (1 + y / 7))))))
    return jnp.where(y > -0.35, series, jnp.exp(y) - 1.0)


def softplus_neg(x):
    u = jnp.exp(-jnp.abs(x))
    series = u * (1 - u * (1 / 2 - u * (1 / 3 - u * (1 / 4 - u * (1 / 5 - u / 6)))))
    return jnp.maximum(-x, 0.0) + jnp.where(u < 0.05, series, jnp.log(1.0 + u))


def layer_kernel(
    ep, tp, top,
    count, *refs,
):
    small_hbm, large, small = refs[:count], refs[count:-count], refs[-count:]
    layer_body(ep, tp, top, small_hbm, small, *large)


def layer_body(
    ep, tp, top, small_hbm, small,
    rows_hbm, tokens_hbm, ip_hbm, gp_hbm, op_hbm, eg_hbm, eu_hbm, ed, sg_hbm, su_hbm, sd_hbm,
    mo_hbm, eo_hbm,
    outq, normed, en, e_out, r_out, r_near,
    w1, eg, eu, wd, sd, recv, hid, ret, back, mt, st, m_half, e_half, m_out, m_in, e_in,
    r_buf, r_in, total, gate, a_buf, b_buf, ext, ends, got, gated, meta, cols_ref, mo_ref, eo_ref,
    load_sem, small_sem, out_sem, halo_send, halo_recv, end_send, end_recv,
    z_s, z_r, y_s, y_r, c_s, c_r, hy_s, hy_r, hc_s, hc_r, w_s, w_r, b_s, b_r,
    md_s, md_r, ed_s, ed_r, my_s, my_r, ey_s, ey_r, r_s, r_r, l_s, l_r,
):
    ids_ref, weights_ref, xg_ref, taps_ref, ig_ref, dg_ref, offset_ref, mg_ref, ms_ref, es_ref = small
    me, t = lax.axis_index("ep"), lax.axis_index("tp")
    ys = tp // 2
    y, c = t // 2, lax.rem(t, 2)
    mate = y * 2 + 1 - c
    dq = outq.shape[3]
    cap = outq.shape[2]
    rows, width = ext.shape[0] - halo_rows, ext.shape[1]
    each = rows // tp
    blocks, bw = ig_ref.shape[0], ig_ref.shape[1]
    sh_width = sd.shape[0]
    half, quarter = ep // 2, ep // 4
    sizes = [2] * quarter + [1] * half
    groups, first_far = quarter + half, quarter
    inner = lax.rem(me // quarter + 1, 4) // 2

    def at_y(k):
        return lax.rem(y + k, ys)

    def up(k):
        return at_y(k) * 2 + c

    def down_of(k, core):
        return lax.rem(y + ys - k, ys) * 2 + core

    def partner(i):
        out, bit = 0, 1
        while bit < ep:
            out = out + lax.rem(me // bit + i // bit, 2) * bit
            bit *= 2
        return out

    def far(j):
        return half + lax.rem(j + inner * quarter, half)

    def base_of(g):
        start = sum(sizes[:g])
        return start if start < half else far(start - half)

    def span_of(g):
        return pl.ds(base_of(g), sizes[g])

    def blocks_of(g):
        return [base_of(g) + n for n in range(sizes[g]) if g + n > 0]

    def load(src, dst, at):
        return pltpu.make_async_copy(src, dst, load_sem.at[at])

    peers = [(lax.rem(me + i, ep), t) for i in range(1, ep)] + [
        (me, lax.rem(t + i, tp)) for i in range(1, tp)
    ]
    greet(peers)
    small_loads = [
        pltpu.make_async_copy(src, dst, small_sem.at[n])
        for n, (src, dst) in enumerate(zip(small_hbm, small))
    ]
    tokens_load, rows_load = load(tokens_hbm, en, 0), load(
        rows_hbm, normed.at[pl.ds(halo_rows, rows)], 9 + tp
    )
    ip_load = load(ip_hbm, w1, 1)
    tokens_load.start()
    for one in small_loads[:3]:
        one.start()

    def z_copy(i, yy, near):
        n = yy * half + i if near else ys * half - half + i
        return remote(outq.at[yy, i], recv.at[yy * 2 + c, i], z_s.at[n], z_r.at[n], partner(i), t)

    def y_copy(k, i):
        n = i - half
        part = recv.at[t, i]
        return remote(part, part, y_s.at[k - 1, n], y_r.at[k - 1, n], me, up(k))

    def c_copy(k, i):
        q = down_of(k, c)
        return remote(recv.at[q, i], recv.at[q, i], c_s.at[k, i - 1], c_r.at[k, i - 1], me, mate)

    def hy_copy(k, g):
        part = hid.at[t, span_of(g)]
        return remote(part, part, hy_s.at[k - 1, g], hy_r.at[k - 1, g], me, up(k))

    def hc_copy(k, g):
        part = hid.at[down_of(k, c), span_of(g)]
        return remote(part, part, hc_s.at[k, g], hc_r.at[k, g], me, mate)

    def w_copy(i):
        q = lax.rem(t + i, tp)
        return remote(
            ed.at[:, pl.ds(pl.multiple_of(q * dq, dq), dq)], wd.at[t],
            w_s.at[i - 1], w_r.at[i - 1], me, q,
        )

    def b_copy(i):
        return remote(ret.at[i], back.at[i], b_s.at[i - 1], b_r.at[i - 1], partner(i), t)

    def side(h):
        return pl.ds(h * (dq // 2), dq // 2)

    def side_copy(i, h):
        n, to = (h + 1) * half - 1 + i - half, partner(i)
        cols = (i, slice(None), side(h))
        return remote(ret.at[cols], back.at[cols], b_s.at[n], b_r.at[n], to, t)

    def halo_copy():
        return remote(
            rows_hbm.at[pl.ds(rows - halo_rows, halo_rows)], normed.at[pl.ds(0, halo_rows)],
            halo_send, halo_recv, lax.rem(me + 1, ep), t,
        )

    def end_copy(i):
        n, to = i - 1, lax.rem(me + i, ep)
        return remote(ends, got.at[i], end_send.at[n], end_recv.at[n], to, t)

    def pair(ref, half, s, r, k):
        return remote(ref.at[at_y(k) * 2 + 1 - c], half.at[k], s.at[k], r.at[k], me, mate)

    def my_copy(k):
        return remote(m_out.at[k], m_in.at[k], my_s.at[k - 1], my_r.at[k - 1], me, up(k))

    def ey_copy(k, j):
        s, r = ey_s.at[k - 1, j - 1], ey_r.at[k - 1, j - 1]
        return remote(e_out.at[k, j], e_in.at[k, j], s, r, me, up(k))

    def r_copy(k, h):
        src, dst = r_buf.at[at_y(k) * 2 + 1 - c, :, side(h)], r_near.at[k, :, side(h)]
        return remote(src, dst, r_s.at[k, h], r_r.at[k, h], me, mate)

    def late_copy(k, j, h):
        s, r = l_s.at[k - 1, j, h], l_r.at[k - 1, j, h]
        return remote(r_out.at[k, j, :, side(h)], r_in.at[k, j, :, side(h)], s, r, me, up(k))

    def of_chip(yy):
        return pl.ds(pl.multiple_of(yy * 2 * dq, dq), 2 * dq)

    def of_core(yy, core):
        return pl.ds(pl.multiple_of((yy * 2 + core) * dq, dq), dq)

    def normalize(ref, gain, first):
        def some(r, _):
            at = pl.ds(pl.multiple_of(first + r * 32, 16), 32)
            ref[at, :] = rms_scale(ref[at, :], gain[...]).astype(bf16)
            return 0

        lax.fori_loop(0, rows // 32, some, 0)

    for one in small_loads[:3]:
        one.wait()
    member = lax.broadcasted_iota(jnp.int32, (ep, rows), 0)
    chosen = [
        (jnp.bitwise_xor(ids_ref[k : k + 1, :], me) == member).astype(f32) for k in range(top)
    ]
    named = chosen[0]
    for k in range(1, top):
        named = named + chosen[k]
    before = lax.broadcasted_iota(jnp.int32, (rows, rows), 0) < lax.broadcasted_iota(
        jnp.int32, (rows, rows), 1
    )
    earlier = jnp.dot(
        named.astype(bf16), before.astype(f32).astype(bf16), preferred_element_type=f32
    )
    spots = earlier + member.astype(f32) * cap
    meta[...] = jnp.zeros_like(meta)
    for k in range(top):
        meta[k : k + 1, :] = jnp.sum(chosen[k] * spots, axis=0, keepdims=True)
        meta[top + k : top + k + 1, :] = weights_ref[k : k + 1, :]
    cols_ref[...] = meta[...].T

    tokens_load.wait()
    rows_load.start()
    for one in small_loads[3:]:
        one.start()
    ip_load.start()
    normalize(en, xg_ref, 0)
    meet(len(peers))
    halo_copy().start()
    for i in range(1, tp):
        w_copy(i).start()
    eg_load, eu_load = load(eg_hbm, eg, 2), load(eu_hbm, eu, 3)
    eg_load.start()
    eu_load.start()
    wd_load = load(ed.at[:, pl.ds(pl.multiple_of(t * dq, dq), dq)], wd.at[t], 4)
    wd_load.start()
    sd_load = load(sd_hbm, sd, 5)
    sd_load.start()
    mine = pl.ds(pl.multiple_of(t * dq, dq), dq)

    def place(i):
        spot = (lax.broadcasted_iota(jnp.int32, (cap, rows), 0) + i * cap).astype(f32)
        hot = meta[0:1, :] == spot
        for k in range(1, top):
            hot = hot | (meta[k : k + 1, :] == spot)
        return hot.astype(f32).astype(bf16)

    def dispatch_near(i, _):
        hot = place(i)
        for yy in range(ys):
            part = pl.ds(pl.multiple_of((yy * 2 + c) * dq, dq), dq)
            outq[yy, i] = jnp.dot(hot, en[:, part], preferred_element_type=f32).astype(bf16)
            z_copy(i, yy, True).start()
        return 0

    def dispatch_far(j, _):
        i = far(j)
        outq[y, i] = jnp.dot(place(i), en[:, mine], preferred_element_type=f32).astype(bf16)
        z_copy(i, y, False).start()
        return 0

    def dispatch_fars(when, lo, hi):
        @pl.when(inner == when)
        def _():
            lax.fori_loop(lo, hi, dispatch_far, 0)

    def dispatch_nears(when, lo, hi):
        @pl.when(inner == when)
        def _():
            lax.fori_loop(lo, hi, dispatch_near, 0)

    lax.fori_loop(1, quarter, dispatch_near, 0)
    dispatch_fars(1, 0, quarter)
    lax.fori_loop(quarter, half - 1, dispatch_near, 0)
    local = place(0)
    for q in range(tp):
        recv[q, 0] = jnp.dot(
            local, en[:, pl.ds(q * dq, dq)], preferred_element_type=f32
        ).astype(bf16)
    dispatch_fars(1, quarter, half - 1)
    for one in small_loads[3:]:
        one.wait()
    rows_load.wait()
    normalize(normed, mg_ref, halo_rows)
    halo_copy().wait_recv()
    normed[pl.ds(0, halo_rows), :] = rms_scale(
        normed[pl.ds(0, halo_rows), :], mg_ref[...]
    ).astype(bf16)
    sg_load = load(sg_hbm, w1.at[:, pl.ds(0, sh_width)], 6)
    su_load = load(su_hbm, w1.at[:, pl.ds(sh_width, sh_width)], 7)
    gp_load = load(gp_hbm, w1, 8)
    op_loads = [
        load(op_hbm.at[:, pl.ds(q * dq, dq)], w1.at[pl.ds(q * width, width), :], 9 + q)
        for q in range(tp)
    ]

    def project():
        ip_load.wait()

        def columns(j, _):
            cols = pl.ds(pl.multiple_of(j * bw, bw), bw)
            piece = jnp.dot(normed[...], w1[:, cols], preferred_element_type=f32)
            ext[:, cols] = piece.astype(bf16).astype(f32)
            return 0

        lax.fori_loop(0, width // bw, columns, 0)
        gp_load.start()

        @pl.when(me == 0)
        def _():
            ext[pl.ds(0, halo_rows), :] = jnp.zeros((halo_rows, width), f32)

    def shared():
        sg_load.wait()
        su_load.wait()
        g = jnp.dot(en[...], w1[:, pl.ds(0, sh_width)], preferred_element_type=f32)
        u = jnp.dot(en[...], w1[:, pl.ds(sh_width, sh_width)], preferred_element_type=f32)
        hidden = (jax.nn.silu(g) * u).astype(bf16)
        for one in op_loads:
            one.start()
        sd_load.wait()
        for q in range(tp):
            cols = pl.ds(q * dq, dq)
            piece = jnp.dot(hidden, sd[:, cols], preferred_element_type=f32)
            st[:, :, cols] = piece.reshape(tp, each, dq)
        for k in range(ys):
            pair(st, e_half, ed_s, ed_r, k).start()

    def gate_step():
        gp_load.wait()

        def columns(j, _):
            cols = pl.ds(pl.multiple_of(j * bw, bw), bw)
            piece = jnp.dot(
                normed[pl.ds(halo_rows, rows)], w1[:, cols], preferred_element_type=f32
            )
            gate[:, cols] = jax.nn.gelu(piece)
            return 0

        lax.fori_loop(0, width // bw, columns, 0)
        sg_load.start()
        su_load.start()

    def convolve():
        taps = taps_ref.shape[0]
        base = halo_rows - (taps - 1)
        first = (lax.broadcasted_iota(jnp.int32, (rows, bw), 0) == 0) & (me == 0)
        for b in range(blocks):
            cols = pl.ds(b * bw, bw)
            acc = taps_ref[0:1, cols] * ext[pl.ds(base, rows), cols]
            for k in range(1, taps):
                acc = acc + taps_ref[k : k + 1, cols] * ext[pl.ds(base + k, rows), cols]
            conv = acc.astype(bf16)
            ig = jax.nn.sigmoid(jnp.dot(conv, ig_ref[b], preferred_element_type=f32))
            dg = jax.nn.sigmoid(jnp.dot(conv, dg_ref[b], preferred_element_type=f32))
            ld = -lru_power * dg * softplus_neg(offset_ref[0:1, cols])
            scale = jnp.where(first, 1.0, jnp.sqrt(-expm1_neg(2.0 * ld)))
            a_buf[:, cols] = jnp.exp(ld)
            b_buf[:, cols] = scale * ig * conv.astype(f32)

    def scan():
        row = lax.broadcasted_iota(jnp.int32, (8, width), 0)

        def block(r, carry):
            pc, sc = carry
            at = pl.ds(pl.multiple_of(r * 8, 8), 8)
            a, b = a_buf[at, :], b_buf[at, :]
            for sh in (1, 2, 4):
                keep = row >= sh
                b = jnp.where(keep, b + a * pltpu.roll(b, sh, 0), b)
                a = jnp.where(keep, a * pltpu.roll(a, sh, 0), a)
            b = b + a * sc
            a = a * pc
            a_buf[at, :] = a
            b_buf[at, :] = b
            return a[7:8, :], b[7:8, :]

        pl_last, s_last = lax.fori_loop(
            0, rows // 8, block, (jnp.ones((1, width), f32), jnp.zeros((1, width), f32))
        )
        ends[...] = jnp.where(row == 0, pl_last, s_last)
        for i in range(1, ep):
            end_copy(i).start()

    def carry_in():
        for i in range(1, ep):
            end_copy(i).wait()
        carry = jnp.zeros((1, width), f32)
        for i in range(ep - 1, 0, -1):
            carry = jnp.where(me >= i, got[i, 0:1, :] * carry + got[i, 1:2, :], carry)

        def finish(r, _):
            at = pl.ds(pl.multiple_of(r * 16, 16), 16)
            gated[at, :] = (gate[at, :] * (b_buf[at, :] + a_buf[at, :] * carry)).astype(bf16)
            return 0

        lax.fori_loop(0, rows // 16, finish, 0)

    def project_out():
        for one in op_loads:
            one.wait()
        for q in range(tp):
            piece = jnp.dot(
                gated[...], w1[pl.ds(q * width, width), :], preferred_element_type=f32
            )
            mt[:, :, pl.ds(q * dq, dq)] = piece.reshape(tp, each, dq)

    def shared_half():
        for k in range(1, ys):
            pair(st, e_half, ed_s, ed_r, k).wait_recv()
            for j in range(1, ys):
                cols = of_chip(at_y(j))
                e_out[k, j] = (e_half[k, :, cols] + st[up(k), :, cols]).astype(bf16)
                ey_copy(k, j).start()

    def mixer_half():
        for k in range(1, ys):
            pair(mt, m_half, md_s, md_r, k).wait_recv()
            m_out[k] = (m_half[k] + mt[up(k)]).astype(bf16)
            my_copy(k).start()

    def arrive(g):
        for i in blocks_of(g):
            if g < first_far:
                for yy in range(ys):
                    z_copy(i, yy, True).wait_recv()
                for k in range(ys):
                    c_copy(k, i).start()
            else:
                z_copy(i, y, False).wait_recv()
                for k in range(1, ys):
                    y_copy(k, i).start()
                c_copy(0, i).start()

    def forward(g):
        if g >= first_far:
            for i in blocks_of(g):
                for k in range(1, ys):
                    y_copy(k, i).wait_recv()
                    c_copy(k, i).start()

    def feed(g):
        for i in blocks_of(g):
            for k in range(ys):
                c_copy(k, i).wait_recv()
        both = span_of(g)
        gate_sum = up_sum = None
        for q in range(tp):
            x = recv[q, both].reshape(sizes[g] * cap, dq)
            span = pl.ds(q * dq, dq)
            g_part = jnp.dot(x, eg[span, :], preferred_element_type=f32)
            u_part = jnp.dot(x, eu[span, :], preferred_element_type=f32)
            gate_sum = g_part if gate_sum is None else gate_sum + g_part
            up_sum = u_part if up_sum is None else up_sum + u_part
        hidden = (jax.nn.silu(gate_sum) * up_sum).astype(bf16)
        hid[t, both] = hidden.reshape(sizes[g], cap, hidden.shape[1])
        for k in range(1, ys):
            hy_copy(k, g).start()
        hc_copy(0, g).start()

    def pass_on(g):
        for k in range(1, ys):
            hy_copy(k, g).wait_recv()
            hc_copy(k, g).start()

    def finish(g):
        for k in range(ys):
            hc_copy(k, g).wait_recv()
        both = span_of(g)
        out = None
        for q in range(tp):
            h = hid[q, both].reshape(sizes[g] * cap, hid.shape[3])
            part = jnp.dot(h, wd[q], preferred_element_type=f32)
            out = part if out is None else out + part
        out = out.astype(bf16).reshape(sizes[g], cap, dq)
        if g == 0:
            back[0] = out[0]
        ret[both] = out
        for i in blocks_of(g):
            if g < first_far:
                b_copy(i).start()
            else:
                side_copy(i, 0).start()
                if g < groups - 2:
                    side_copy(i, 1).start()

    project()
    dispatch_fars(1, half - 1, half)
    dispatch_nears(0, half - 1, half)
    convolve()
    scan()
    gate_step()
    dispatch_nears(1, half - 1, half)
    dispatch_fars(0, 0, quarter)
    arrive(first_far)
    shared()
    dispatch_fars(0, quarter, half)
    arrive(first_far + 1)
    arrive(0)
    eg_load.wait()
    eu_load.wait()
    feed(0)
    wd_load.wait()
    for g in (first_far, first_far + 1):
        forward(g)
        feed(g)
    for i in range(1, tp):
        w_copy(i).wait()
    for g in (first_far, first_far + 1):
        pass_on(g)
        finish(g)
    for g in range(1, first_far):
        arrive(g)
        feed(g)
    last = groups - 2
    for g in range(first_far + 2, last):
        arrive(g)
        forward(g)
        feed(g)
        pass_on(g)
        finish(g)
    arrive(last)
    pass_on(0)
    finish(0)
    arrive(last + 1)
    for near in range(1, first_far):
        pass_on(near)
        finish(near)
    forward(last)
    feed(last)
    carry_in()
    project_out()
    forward(last + 1)
    feed(last + 1)
    pass_on(last)
    finish(last)
    pass_on(last + 1)
    for k in range(ys):
        pair(mt, m_half, md_s, md_r, k).start()
    shared_half()
    finish(last + 1)
    mixer_half()
    for g in (last, last + 1):
        for i in blocks_of(g):
            side_copy(i, 0).wait_send()
            side_copy(i, 1).start()

    def combine(lo, count, cols):
        flat = back[pl.ds(lo, count), :, cols].reshape(count * cap, -1)
        spot = (lax.broadcasted_iota(jnp.int32, (rows, count * cap), 1) + lo * cap).astype(f32)
        out = None
        for k in range(top):
            pick = (cols_ref[:, k : k + 1] == spot).astype(f32).astype(bf16)
            term = cols_ref[:, top + k : top + k + 1] * jnp.dot(
                pick, flat, preferred_element_type=f32
            )
            out = term if out is None else out + term
        return out.reshape(tp, each, -1)

    for i in range(1, half):
        b_copy(i).wait_recv()
    r_buf[...] = combine(0, half, pl.ds(0, dq))
    pair(st, e_half, ed_s, ed_r, 0).wait_recv()
    total[...] = e_half[0] + st[t]
    for k in range(1, ys):
        for j in range(1, ys):
            ey_copy(k, j).wait_recv()
            cols = of_chip(lax.rem(y + ys - k + j, ys))
            total[:, cols] = total[:, cols] + e_in[k, j].astype(f32)
    near = of_core(y, 1 - c)

    def part_of(q, h):
        return pl.ds(pl.multiple_of(q * dq + h * dq // 2, dq // 2), dq // 2)

    for h in range(2):
        cols, mine_h, near_h = side(h), part_of(t, h), part_of(mate, h)
        for i in range(half, ep):
            side_copy(i, h).wait_recv()
        r_buf[:, :, cols] = r_buf[:, :, cols] + combine(half, half, cols)
        for k in range(ys):
            r_copy(k, h).start()
        for k in range(1, ys):
            r_out[k, 0, :, cols] = (
                e_half[k, :, mine_h] + st[up(k), :, mine_h] + r_buf[up(k), :, cols]
            ).astype(bf16)
            late_copy(k, 0, h).start()
        for k in range(1, ys):
            r_copy(k, h).wait_recv()
            r_out[k, 1, :, cols] = (
                e_half[k, :, near_h] + st[up(k), :, near_h] + r_near[k, :, cols]
            ).astype(bf16)
            late_copy(k, 1, h).start()
    pair(mt, m_half, md_s, md_r, 0).wait_recv()
    whole = m_half[0] + mt[t]
    for k in range(1, ys):
        my_copy(k).wait_recv()
        whole = whole + m_in[k].astype(f32)
    mo_ref[...] = rms_scale(whole, ms_ref[...]).astype(bf16)
    mo_store = pltpu.make_async_copy(mo_ref, mo_hbm, out_sem.at[0])
    mo_store.start()
    total[:, mine] = total[:, mine] + r_buf[t]
    for h in range(2):
        r_copy(0, h).wait_recv()
    total[:, near] = total[:, near] + r_near[0]
    for k in range(1, ys):
        for j in range(2):
            for h in range(2):
                late_copy(k, j, h).wait_recv()
            cols = of_core(lax.rem(y + ys - k, ys), lax.rem(c + j, 2))
            total[:, cols] = total[:, cols] + r_in[k, j].astype(f32)
    eo_ref[...] = rms_scale(total[...], es_ref[...]).astype(bf16)
    eo_store = pltpu.make_async_copy(eo_ref, eo_hbm, out_sem.at[1])
    eo_store.start()

    def settle_near(i, _):
        for yy in range(ys):
            z_copy(i, yy, True).wait_send()
        for k in range(ys):
            c_copy(k, i).wait_send()
        b_copy(i).wait_send()
        return 0

    def settle_far(i, _):
        z_copy(i, y, False).wait_send()
        for k in range(1, ys):
            y_copy(k, i).wait_send()
        for k in range(ys):
            c_copy(k, i).wait_send()
        return 0

    for g in range(first_far, groups):
        for i in blocks_of(g):
            if g < groups - 2:
                side_copy(i, 0).wait_send()
            side_copy(i, 1).wait_send()
    halo_copy().wait_send()
    lax.fori_loop(1, half, settle_near, 0)
    lax.fori_loop(half, ep, settle_far, 0)
    for g in range(groups):
        for k in range(1, ys):
            hy_copy(k, g).wait_send()
        for k in range(ys):
            hc_copy(k, g).wait_send()
    for k in range(ys):
        pair(mt, m_half, md_s, md_r, k).wait_send()
        pair(st, e_half, ed_s, ed_r, k).wait_send()
    for k in range(ys):
        for h in range(2):
            r_copy(k, h).wait_send()
    for k in range(1, ys):
        my_copy(k).wait_send()
        for j in range(1, ys):
            ey_copy(k, j).wait_send()
        for j in range(2):
            for h in range(2):
                late_copy(k, j, h).wait_send()
    mo_store.wait()
    eo_store.wait()


def dma(*shape):
    return pltpu.SemaphoreType.DMA(shape)


def layer(ep, tp, small, large):
    rows, depth = large[0].shape
    width = large[2].shape[1]
    hf, hs = large[5].shape[1], large[8].shape[1]
    top = small[0].shape[0]
    each, ys, dq = rows // tp, tp // 2, depth // tp
    groups = ep // 4 + ep // 2
    cap = rows * top * 3 // (2 * ep)
    V = pltpu.VMEM
    return pl.pallas_call(
        functools.partial(layer_kernel, ep, tp, top, len(small)),
        out_shape=[jax.ShapeDtypeStruct((each, depth), bf16)] * 2,
        in_specs=[pl.BlockSpec(memory_space=pl.ANY)] * (len(small) + len(large)),
        out_specs=[pl.BlockSpec(memory_space=pl.ANY)] * 2,
        scratch_shapes=[
            V((ys, ep, cap, dq), bf16),
            V((halo_rows + rows, depth), bf16),
            V((rows, depth), bf16),
            V((ys, ys, each, 2 * dq), bf16),
            V((ys, 2, each, dq), bf16),
            V((ys, each, dq), f32),
            V((depth, width), bf16),
            V((depth, hf), bf16),
            V((depth, hf), bf16),
            V((tp, hf, dq), bf16),
            V((hs, depth), bf16),
            V((tp, ep, cap, dq), bf16),
            V((tp, ep, cap, hf), bf16),
            V((ep, cap, dq), bf16),
            V((ep, cap, dq), bf16),
            V((tp, each, depth), f32),
            V((tp, each, depth), f32),
            V((ys, each, depth), f32),
            V((ys, each, depth), f32),
            V((ys, each, depth), bf16),
            V((ys, each, depth), bf16),
            V((ys, ys, each, 2 * dq), bf16),
            V((tp, each, dq), f32),
            V((ys, 2, each, dq), bf16),
            V((each, depth), f32),
            V((rows, width), f32),
            V((rows, width), f32),
            V((rows, width), f32),
            V((halo_rows + rows, width), f32),
            V((8, width), f32),
            V((ep, 8, width), f32),
            V((rows, width), bf16),
            V((128, rows), f32),
            V((rows, 128), f32),
            V((each, depth), bf16),
            V((each, depth), bf16),
            dma(10 + tp), dma(len(small)), dma(2), pltpu.SemaphoreType.DMA, pltpu.SemaphoreType.DMA,
            dma(ep - 1), dma(ep - 1),
            dma((ys + 1) * ep // 2), dma((ys + 1) * ep // 2),
            dma(ys - 1, ep // 2), dma(ys - 1, ep // 2),
            dma(ys, ep - 1), dma(ys, ep - 1),
            dma(ys - 1, groups), dma(ys - 1, groups),
            dma(ys, groups), dma(ys, groups),
            dma(tp - 1), dma(tp - 1),
            dma(ep + ep // 2 - 1), dma(ep + ep // 2 - 1),
            dma(ys), dma(ys), dma(ys), dma(ys),
            dma(ys - 1), dma(ys - 1), dma(ys - 1, ys - 1), dma(ys - 1, ys - 1),
            dma(ys, 2), dma(ys, 2), dma(ys - 1, 2, 2), dma(ys - 1, 2, 2),
        ]
        + [V(x.shape, x.dtype) for x in small],
        compiler_params=pltpu.CompilerParams(
            collective_id=0, has_side_effects=True, vmem_limit_bytes=67000000
        ),
        name="layer",
    )(*small, *large)


def publish_kernel(mixer, expert, mixer_out, expert_out):
    mixer_out[...] = mixer[...]
    expert_out[...] = expert[...]


def publish(mixer, expert):
    return pl.pallas_call(
        publish_kernel,
        out_shape=[jax.ShapeDtypeStruct(x.shape, x.dtype) for x in (mixer, expert)],
        in_specs=[pl.BlockSpec(memory_space=pltpu.VMEM)] * 2,
        out_specs=[pl.BlockSpec(memory_space=pltpu.VMEM)] * 2,
        name="publish",
    )(mixer, expert)


def body(
    mixer_rows, mixer_gain, gate_proj, input_proj, conv_taps, input_gates, decay_gates,
    decay_offset, out_proj, mixer_scale, expert_rows, expert_gain, route_ids, route_weights,
    expert_gate, expert_up, expert_down, shared_gate, shared_up, shared_down, expert_scale,
):
    ep, tp = lax.axis_size("ep"), lax.axis_size("tp")
    gains = [x.reshape(1, -1) for x in (mixer_gain, expert_gain, mixer_scale, expert_scale)]
    small = (
        route_ids.T, route_weights.T, gains[1], conv_taps, input_gates, decay_gates,
        decay_offset.reshape(1, -1), gains[0], gains[2], gains[3],
    )
    large = (
        mixer_rows, expert_rows, input_proj, gate_proj, out_proj, expert_gate[0], expert_up[0], expert_down[0],
        shared_gate, shared_up, shared_down,
    )
    return tuple(publish(*layer(ep, tp, small, large)))


def solution(mesh):
    placed = (
        P("ep", None),
        P(),
        P(None, "tp"),
        P(None, "tp"),
        P(None, "tp"),
        P("tp", None, None),
        P("tp", None, None),
        P("tp"),
        P("tp", None),
        P(),
        P("ep", None),
        P(),
        P("ep", None),
        P("ep", None),
        P("ep", None, "tp"),
        P("ep", None, "tp"),
        P("ep", "tp", None),
        P(None, "tp"),
        P(None, "tp"),
        P("tp", None),
        P(),
    )
    return jax.shard_map(
        body,
        mesh=mesh,
        in_specs=placed,
        out_specs=(P(("ep", "tp"), None), P(("ep", "tp"), None)),
        check_vma=False,
    )
```
